512 devices in a mesh: ep: 32 (over z, core), tp: 16 (over y, x).
Axes of the slice: x: 4, y: 4, z: 16, core: 2. Of those that a mesh axis runs over, the one named last changes fastest.
Arguments:
- receptance: bfloat16 [8192, 2048], P('ep', 'tp'), may hold values from -6 to 6
- key_in: bfloat16 [8192, 2048], P('ep', 'tp'), may hold values from -6 to 6
- value_in: bfloat16 [8192, 2048], P('ep', 'tp'), may hold values from -6 to 6
- decay_in: bfloat16 [8192, 2048], P('ep', 'tp'), may hold values from -16 to 2
- rate_in: bfloat16 [8192, 2048], P('ep', 'tp'), may hold values from -12 to 4
- norm_gain: float32 [2048], P('tp'), may hold values from 0.1 to 1.9
- out_weight: bfloat16 [2048, 4096], P('tp'), may hold values from -0.125 to 0.125
- moe_in: bfloat16 [4096, 4096], P('ep'), may hold values from -6 to 6
- ffn_gain: float32 [4096], replicated, may hold values from 0.1 to 1.9
- routes: int32 [4096, 4], P('ep'), may hold values from 0 to 31, all different within a row; in each aligned block of 128 rows (0 to 127, 128 to 255, ...) at most 20 rows name the same one
- route_weights: float32 [4096, 4], P('ep'), may hold values from 0.2 to 1
- gate_weight: bfloat16 [32, 4096, 1024], P('ep', None, 'tp'), may hold values from -0.09375 to 0.09375
- up_weight: bfloat16 [32, 4096, 1024], P('ep', None, 'tp'), may hold values from -0.09375 to 0.09375
- down_weight: bfloat16 [32, 1024, 4096], P('ep', None, 'tp'), may hold values from -0.1875 to 0.1875
Outputs:
- mixer_out: bfloat16 [8192, 4096], P(('ep', 'tp'))
- moe_out: bfloat16 [4096, 4096], P('ep', 'tp')
The draws below stay inside these ranges and needn't reach their ends.
Inputs may be any that keep to these rules, and one draw needn't show every extreme that they name: `routes`: A row names 4 different experts. Among the 128 rows that one index of ep holds, no expert is named by more than 20 rows, and in every draw some expert is named by exactly 20 of them.
All inputs are finite; a program needn't handle non-finite values.
Results may differ from the reference program's by a relative error of at most 0.025.
Values may be sent and summed in bfloat16 or wider, within the bound.
No kernel may reach another device: no remote copies, remote signals or barrier semaphores. Data moves between devices by JAX's collectives and lax.ppermute only.
A program may use at most 64 MiB of HBM per device.

```python
import math
import jax
import jax.numpy as jnp
import numpy as np
from jax import lax

D = 4096
HEADS = 32
HD = 64
FE = 1024
TOPK = 4
TOK_DEV = 256
R_DEV = 128
WIDTH = 2048
TOKENS = 8192
MOE_ROWS = 4096
EXPERTS = 32
CAP = 20
N_EP = 32
N_TP = 16


def slow_heads(key):
    chance = 0.5
    return jax.random.uniform(jax.random.fold_in(key, 11), (HEADS,)) < chance


def span_offsets(key, salt, reach):
    span_count = TOKENS // TOK_DEV
    offsets = jax.random.uniform(jax.random.fold_in(key, salt), (span_count, HEADS), jnp.float32, -reach, reach)
    return jnp.repeat(offsets, TOK_DEV, axis=0)[:, :, None]


def jitter(key, salt, spread):
    shape = (TOKENS, HEADS, HD)
    return jax.random.normal(jax.random.fold_in(key, salt), shape, jnp.float32) * spread


def draw_decay_in(key, part):
    slow = slow_heads(key)
    level = jnp.where(slow, math.log(0.5 / TOKENS) + 0.5, math.log(1.0 / 40.0) + 0.5).astype(jnp.float32)
    values = level[None, :, None] + span_offsets(key, 12, 1.0) + jitter(key, 13, 0.5)
    return jnp.clip(values, -16.0, 2.0).reshape(TOKENS, HEADS * HD).astype(jnp.bfloat16)


def draw_rate_in(key, part):
    slow = slow_heads(key)
    level = jnp.where(slow, math.log(0.5 * HD / TOKENS), 0.0).astype(jnp.float32)
    spread = jnp.where(slow, 0.5, 1.0).astype(jnp.float32)[None, :, None]
    values = level[None, :, None] + span_offsets(key, 14, 0.7) + jitter(key, 15, 1.0) * spread
    return jnp.clip(values, -12.0, 4.0).reshape(TOKENS, HEADS * HD).astype(jnp.bfloat16)


def block_levels(rng, extent, split, low, high):
    loudness, own = 1.0, jax.random.fold_in(rng, 6)
    for axis_at, parts in split:
        heights = jnp.exp(jax.random.uniform(jax.random.fold_in(own, axis_at), (parts,), jnp.float32, low / len(split), high / len(split)))
        loudness = loudness * jnp.repeat(heights, extent[axis_at] // parts).reshape([-1 if axis == axis_at else 1 for axis in range(len(extent))])
    return loudness


def routed_block(stream_key, own, number, rows, number_of, top, bound, slope):
    sequence = jax.random.permutation(stream_key, number_of)
    heavy_load, common = shares(number_of, rows * top, bound, slope, True), shares(number_of, rows * top, bound, slope, False)
    places = jnp.arange(number_of)

    def named(sizes, rotation):
        used = int((sizes > 0).sum())
        fixed = max(1, used // 4)
        moved = fixed + (places - fixed + rotation * (used - fixed)) % max(1, number_of - fixed)
        return jnp.zeros((number_of,), jnp.int32).at[sequence[jnp.where(places < fixed, places, moved)]].set(jnp.asarray(sizes, jnp.int32))

    sizes = jnp.where(number % 4 == 0, named(heavy_load, number // 4), named(common, number - number // 4 - 1))
    mixed = jax.random.permutation(jax.random.fold_in(own, 3), number_of)
    giver, sink = mixed[0:number_of // 2 * 2:2], mixed[1:number_of // 2 * 2:2]
    margin = jnp.minimum(sizes[giver] - 1, bound - sizes[sink]) // 2
    margin = jnp.where((giver == sequence[0]) | (sink == sequence[0]) | (sizes[sink] == 0), 0, jnp.maximum(margin, 0))
    moved = jax.random.randint(jax.random.fold_in(own, 4), (number_of // 2,), 0, 1 << 20) % (margin + 1)
    sizes = sizes.at[giver].add(-moved).at[sink].add(moved)
    members = jnp.searchsorted(jnp.cumsum(sizes), jnp.arange(rows * top), side="right").astype(jnp.int32)
    table = members.reshape(top, rows).T
    table = table[jax.random.permutation(jax.random.fold_in(own, 1), rows)]
    rotation = jax.random.randint(jax.random.fold_in(own, 2), (rows, 1), 0, top)
    return jnp.take_along_axis(table, (jnp.arange(top)[None, :] + rotation) % top, axis=1)


def shares(count, total, limit, slope, full):
    weights = [(1 << 20) // math.isqrt(rank ** slope) + 1 for rank in range(1, count + 1)]
    largest = limit if full else min(limit, max(-(-total // count), total * weights[0] // sum(weights)))
    least = 1 if total - largest >= count - 1 else 0
    given, surplus = [largest] + [least] * (count - 1), total - largest - least * (count - 1)
    while surplus > 0:
        movable = [i for i in range(1, count) if given[i] < largest] or [i for i in range(1, count) if given[i] < limit]
        pool, remaining = sum([weights[i] for i in movable]), surplus
        for i in movable:
            addition = min(limit - given[i], max(1, remaining * weights[i] // pool), surplus)
            given[i] = given[i] + addition
            surplus = surplus - addition
    return np.array(given)


def scatter_about(rng, dims, width, most, cuts=(), held_as=jnp.bfloat16):
    values = jax.random.normal(rng, dims, jnp.float32) * width
    if len(cuts) > 0:
        values = block_levels(rng, dims, cuts, -0.22, 0.18) * values
    return jnp.clip(values, min=-most, max=most).astype(held_as)


def setup_inputs(seed: int = 0) -> dict:
    seeds = jax.random.split(jax.random.key(seed), 15)
    receptance = scatter_about(seeds[0], (TOKENS, WIDTH), 1.0, 6.0, ((0, 32), (1, 16)))
    key_in = scatter_about(seeds[1], (TOKENS, WIDTH), 1.0, 6.0, ((0, 32), (1, 16)))
    value_in = scatter_about(seeds[2], (TOKENS, WIDTH), 1.0, 6.0, ((0, 32), (1, 16)))
    decay_in = draw_decay_in(jax.random.fold_in(seeds[14], 71), 0)
    rate_in = draw_rate_in(jax.random.fold_in(seeds[14], 71), 0)
    norm_gain = jnp.clip(1.0 + 0.18 * jax.random.normal(seeds[5], (WIDTH,), jnp.float32), 0.1, 1.9)
    out_weight = scatter_about(seeds[6], (WIDTH, D), WIDTH ** -0.5, 0.125, ((0, 16),))
    moe_in = scatter_about(seeds[7], (MOE_ROWS, D), 1.0, 6.0, ((0, 32),))
    ffn_gain = jnp.clip(1.0 + 0.18 * jax.random.normal(seeds[8], (D,), jnp.float32), 0.1, 1.9)
    routes_keys = jax.random.split(jax.random.fold_in(seeds[9], 1), MOE_ROWS // R_DEV)
    routes_turns = jax.random.permutation(jax.random.fold_in(seeds[9], 3), MOE_ROWS // R_DEV)
    routes = jax.vmap(lambda own, number: routed_block(jax.random.fold_in(seeds[9], 2), own, number, R_DEV, EXPERTS, TOPK, CAP, 1))(routes_keys, routes_turns).reshape((MOE_ROWS, TOPK))
    route_weights = jnp.clip(0.2 + 0.8 * jax.random.uniform(seeds[10], (MOE_ROWS, TOPK), jnp.float32) ** block_levels(seeds[10], (MOE_ROWS, TOPK), ((0, 32),), -0.2, 0.2), 0.2, 1.0)
    gate_weight = scatter_about(seeds[11], (EXPERTS, D, FE), D ** -0.5, 0.09375, ((0, 32), (2, 16)))
    up_weight = scatter_about(seeds[12], (EXPERTS, D, FE), D ** -0.5, 0.09375, ((0, 32), (2, 16)))
    down_weight = scatter_about(seeds[13], (EXPERTS, FE, D), FE ** -0.5, 0.1875, ((0, 32), (2, 16)))
    return {"receptance": receptance, "key_in": key_in, "value_in": value_in, "decay_in": decay_in, "rate_in": rate_in, "norm_gain": norm_gain, "out_weight": out_weight, "moe_in": moe_in, "ffn_gain": ffn_gain, "routes": routes, "route_weights": route_weights, "gate_weight": gate_weight, "up_weight": up_weight, "down_weight": down_weight}


EXACT_MATMUL = lax.Precision.HIGHEST

def mixer_reference(receptance, key_in, value_in, decay_in, rate_in, norm_gain, out_weight):
    shape = (TOKENS, HEADS, HD)
    readout = receptance.astype(jnp.float32).reshape(shape)
    key_rows = key_in.astype(jnp.float32).reshape(shape)
    value_rows = value_in.astype(jnp.float32).reshape(shape)
    log_decay = -jnp.exp(-jax.nn.softplus(-decay_in.astype(jnp.float32)) - 0.5).reshape(shape)
    learn_rate = jax.nn.sigmoid(rate_in.astype(jnp.float32)).reshape(shape)
    unit_key = key_rows / jnp.sqrt(lax.optimization_barrier(jnp.sum(key_rows * key_rows, axis=-1, keepdims=True)) + 1.0)

    def advance(passed_state, inputs):
        current_readout, key_now, value_now, decay_now, rate_now, current_unit_key = inputs
        sequence_walk = jnp.einsum('bw,bwo->bo', current_unit_key, passed_state, precision=EXACT_MATMUL)
        passed_state = jnp.exp(decay_now)[:, :, None] * passed_state - (current_unit_key * rate_now)[:, :, None] * sequence_walk[:, None, :] + (key_now * rate_now)[:, :, None] * value_now[:, None, :]
        return (passed_state, jnp.einsum('bw,bwo->bo', current_readout, passed_state, precision=EXACT_MATMUL))
    start = jnp.zeros((HEADS, HD, HD), jnp.float32)
    _, heads_out = lax.scan(advance, start, (readout, key_rows, value_rows, log_decay, learn_rate, unit_key))
    center = heads_out - lax.optimization_barrier(jnp.mean(heads_out, axis=-1, keepdims=True))
    spread = lax.optimization_barrier(jnp.mean(center * center, axis=-1, keepdims=True))
    normed = center * lax.rsqrt(spread + 1.0) * norm_gain.astype(jnp.float32).reshape(HEADS, HD)
    mixed = normed.reshape(TOKENS, WIDTH).astype(jnp.bfloat16)
    group_width = WIDTH // N_TP

    def add_group(running, group_index):
        columns = lax.dynamic_slice_in_dim(mixed, group_index * group_width, group_width, 1)
        weights = lax.dynamic_slice_in_dim(out_weight, group_index * group_width, group_width, 0)
        product = jnp.dot(columns, weights, preferred_element_type=jnp.float32).astype(jnp.bfloat16)
        product = lax.optimization_barrier(product)
        return (running + product.astype(jnp.float32), None)
    summed, _ = lax.scan(add_group, jnp.zeros((TOKENS, D), jnp.float32), jnp.arange(N_TP, dtype=jnp.int32))
    return summed.astype(jnp.bfloat16)

def expert_reference(moe_in, ffn_gain, routes, route_weights, gate_weight, up_weight, down_weight):
    row_values = moe_in.astype(jnp.float32)
    scaled = row_values * lax.rsqrt(lax.optimization_barrier(jnp.mean(row_values * row_values, axis=-1, keepdims=True)) + 1.0) * ffn_gain
    normed_rows = scaled.astype(jnp.bfloat16)
    pairs = routes.reshape(-1).astype(jnp.int32)
    pair_count = pairs.shape[0]
    onehot = (pairs[:, None] == jnp.arange(EXPERTS, dtype=jnp.int32)[None, :]).astype(jnp.int32)
    slot_rank = lax.optimization_barrier(jnp.sum((jnp.cumsum(onehot, axis=0) - onehot) * onehot, axis=1)).astype(jnp.int32)
    capacity = N_EP * CAP
    position = (pairs * capacity + slot_rank).astype(jnp.int32)
    source = jnp.zeros((EXPERTS * capacity,), jnp.int32).at[position].set(jnp.arange(pair_count, dtype=jnp.int32) // TOPK).reshape(EXPERTS, capacity)
    filled = jnp.zeros((EXPERTS * capacity,), jnp.int32).at[position].set(1).reshape(EXPERTS, capacity)

    def one_expert(operands):
        source_rows, live, gate_matrix, up_matrix, down_matrix = operands
        taken = jnp.where(live[:, None] > 0, normed_rows[source_rows], jnp.zeros((), normed_rows.dtype))
        gate = jnp.dot(taken, gate_matrix, preferred_element_type=jnp.float32)
        up_part = jnp.dot(taken, up_matrix, preferred_element_type=jnp.float32)
        hidden = (jax.nn.silu(gate) * up_part).astype(jnp.bfloat16)
        return jnp.dot(hidden, down_matrix, preferred_element_type=jnp.float32).astype(jnp.bfloat16)
    results = lax.map(one_expert, (source, filled, gate_weight, up_weight, down_weight))
    per_pair = results.reshape(EXPERTS * capacity, D)[position].astype(jnp.float32).reshape(MOE_ROWS, TOPK, D)
    portion = route_weights / lax.optimization_barrier(jnp.sum(route_weights, axis=-1, keepdims=True))
    return lax.optimization_barrier(jnp.sum(portion[:, :, None] * per_pair, axis=1)).astype(jnp.bfloat16)

def reference(receptance, key_in, value_in, decay_in, rate_in, norm_gain, out_weight, moe_in, ffn_gain, routes, route_weights, gate_weight, up_weight, down_weight):
    mixer_out = mixer_reference(receptance, key_in, value_in, decay_in, rate_in, norm_gain, out_weight)
    moe_out = expert_reference(moe_in, ffn_gain, routes, route_weights, gate_weight, up_weight, down_weight)
    return (mixer_out, moe_out)
```

```python
import jax
import jax.numpy as jnp
from jax import lax
from jax.experimental import pallas as pl
from jax.experimental.pallas import tpu as pltpu
from jax.sharding import Mesh
from jax.sharding import PartitionSpec as P

HD = 64
BLOCK = 64
EP = ("ep_0", "ep_1")
TP = ("tp_y", "tp_x")
EP_TP = ("ep_0", "ep_1", "tp_y", "tp_x")
EXPERTS = 32
CAP = 20
SLOT = 2 * CAP
GROUP = 8

EXACT_MATMUL = lax.Precision.HIGHEST


def iota(shape, dim):
    return lax.broadcasted_iota(jnp.int32, shape, dim)


def nt(a, b):
    return lax.dot_general(a, b, (((1,), (1,)), ((), ())), preferred_element_type=jnp.float32)


def mm(a, b):
    return jnp.dot(a, b, preferred_element_type=jnp.float32)


def call(kernel, outs, *args):
    return pl.pallas_call(kernel, out_shape=outs)(*args)


def prep_kernel(x, xs, gain, routes, weights, out, rank_out, share_out):
    rows = x.shape[0]
    full = x[...].astype(jnp.float32)
    scale = lax.rsqrt(jnp.mean(full * full, axis=-1, keepdims=True) + 1.0)
    piece = (xs[...].astype(jnp.float32) * scale * gain[...]).astype(jnp.bfloat16)
    w = weights[...]
    portion = w / jnp.sum(w, axis=-1, keepdims=True)
    expert = iota((rows, EXPERTS), 1)
    chosen = jnp.zeros((rows, EXPERTS), jnp.float32)
    share = jnp.zeros((rows, EXPERTS), jnp.float32)
    for j in range(routes.shape[1]):
        hit = routes[:, j : j + 1] == expert
        chosen = jnp.where(hit, 1.0, chosen)
        share = jnp.where(hit, portion[:, j : j + 1], share)
    earlier = (iota((rows, rows), 1) <= iota((rows, rows), 0)).astype(jnp.bfloat16)
    rank = mm(earlier, chosen.astype(jnp.bfloat16)) * chosen
    rank_out[...] = rank
    share_out[...] = share
    total = EXPERTS * SLOT
    q = iota((total, EXPERTS), 0)
    spread = (q // SLOT == iota((total, EXPERTS), 1)).astype(jnp.bfloat16)
    seat = (iota((total, rows), 0) % CAP + 1).astype(jnp.float32)
    pick = (nt(spread, rank.astype(jnp.bfloat16)) == seat).astype(jnp.bfloat16)
    both = mm(pick, piece)
    second = iota((total, 128), 0) % SLOT >= CAP
    out[...] = jnp.where(second, both[:, 128:], both[:, :128]).astype(jnp.bfloat16)


def combine_kernel(back, rank, share, out):
    rows = rank.shape[0]
    total = EXPERTS * SLOT
    spread = (iota((total, EXPERTS), 0) // SLOT == iota((total, EXPERTS), 1)).astype(jnp.bfloat16)
    q = iota((rows, total), 1)
    match = nt(rank[...].astype(jnp.bfloat16), spread) == (q % CAP + 1).astype(jnp.float32)
    second = q % SLOT >= CAP
    high = share[...].astype(jnp.bfloat16)
    low = (share[...] - high.astype(jnp.float32)).astype(jnp.bfloat16)
    values = back[...]
    first_half = jnp.zeros((rows, 128), jnp.float32)
    second_half = jnp.zeros((rows, 128), jnp.float32)
    for part in (high, low):
        wide = jnp.where(match, nt(part, spread), 0.0)
        first_half += mm(jnp.where(second, 0.0, wide).astype(jnp.bfloat16), values)
        second_half += mm(jnp.where(second, wide, 0.0).astype(jnp.bfloat16), values)
    out[:, :128] = first_half.astype(out.dtype)
    out[:, 128:] = second_half.astype(out.dtype)


def selector(half):
    r = iota((GROUP * CAP, GROUP * SLOT), 0)
    return (iota((GROUP * CAP, GROUP * SLOT), 1) == r // CAP * SLOT + r % CAP + half * CAP).astype(
        jnp.bfloat16
    )


def gate_up_kernel(gathered, weights, out):
    picks = (selector(0), selector(1))
    joined = jnp.concatenate([weights[k] for k in range(weights.shape[0])], axis=1)
    for g in range(EXPERTS // GROUP):
        pieces = []
        for k in range(gathered.shape[0]):
            seen = gathered[k, g * GROUP * SLOT : (g + 1) * GROUP * SLOT, :]
            for pick in picks:
                pieces.append(mm(pick, seen).astype(jnp.bfloat16))
        out[g] = mm(jnp.concatenate(pieces, axis=1), joined).astype(jnp.bfloat16)


def hidden_kernel(parts, out):
    both = jnp.zeros(parts.shape[1:], jnp.float32)
    for k in range(parts.shape[0]):
        both += parts[k].astype(jnp.float32)
    made = []
    for k in range(both.shape[1] // 128):
        v = both[:, k * 128 : (k + 1) * 128]
        made.append(jax.nn.silu(v) * pltpu.roll(v, 64, 1))
    left = iota((both.shape[0], 128), 1) < 64
    for k in range(len(made) // 2):
        out[:, k * 128 : (k + 1) * 128] = jnp.where(
            left, made[2 * k], pltpu.roll(made[2 * k + 1], 64, 1)
        ).astype(jnp.bfloat16)


def down_kernel(hidden, weights, out):
    picks = (selector(0), selector(1))
    side = 4
    tall = []
    for k in range(side):
        tall.append(
            jnp.concatenate(
                [weights[(side * m + k) * 64 : (side * m + k + 1) * 64, :] for m in range(side)], 0
            )
        )
    for g in range(side):
        total = mm(hidden[side * g], tall[0])
        for k in range(1, side):
            total += mm(hidden[side * g + k], tall[k])
        total = total.astype(jnp.bfloat16)
        placed = jnp.zeros((GROUP * SLOT, 128), jnp.float32)
        for half in range(2):
            placed += lax.dot_general(
                picks[half],
                total[:, half * 128 : (half + 1) * 128],
                (((0,), (0,)), ((), ())),
                preferred_element_type=jnp.float32,
            )
        out[g * GROUP * SLOT : (g + 1) * GROUP * SLOT, :] = placed.astype(jnp.bfloat16)


def exchanged(tiles, axis):
    return lax.all_to_all(tiles, axis, split_axis=0, concat_axis=0, tiled=True)


def sent_to_all(shard, axis):
    return exchanged(jnp.broadcast_to(shard, (lax.axis_size(axis), *shard.shape)), axis)


def einsum_exact(form, left, right):
    return jnp.einsum(form, left, right, precision=EXACT_MATMUL)


def block_tables(receptance, key_in, value_in, decay_in, rate_in):
    token_count, columns = receptance.shape
    head_count = columns // HD
    block_count = token_count // BLOCK

    def to_blocks(array):
        return (
            array.astype(jnp.float32)
            .reshape(block_count, BLOCK, head_count, HD)
            .transpose(2, 0, 1, 3)
        )

    readout = to_blocks(receptance)
    key_rows = to_blocks(key_in)
    value_rows = to_blocks(value_in)
    log_decay = -jnp.exp(-jax.nn.softplus(-to_blocks(decay_in)) - 0.5)
    learn_rate = jax.nn.sigmoid(to_blocks(rate_in))
    unit_key = key_rows / jnp.sqrt(jnp.sum(key_rows * key_rows, axis=-1, keepdims=True) + 1.0)
    inclusive = jnp.cumsum(log_decay, axis=2)
    exclusive = inclusive - log_decay
    block_total = inclusive[:, :, -1:, :]
    probe = -unit_key * jnp.exp(exclusive)
    removal = unit_key * learn_rate
    written = key_rows * learn_rate
    removal_back = removal * jnp.exp(-inclusive)
    written_back = written * jnp.exp(-inclusive)
    readout_scaled = readout * jnp.exp(inclusive)
    removal_tail = removal * jnp.exp(block_total - inclusive)
    written_tail = written * jnp.exp(block_total - inclusive)
    strict = jnp.tril(jnp.ones((BLOCK, BLOCK), jnp.float32), -1)
    closed = jnp.tril(jnp.ones((BLOCK, BLOCK), jnp.float32))
    lower = einsum_exact("hbck,hbsk->hbcs", probe, removal_back) * strict
    lower_write = einsum_exact("hbck,hbsk->hbcs", probe, written_back) * strict
    reach = einsum_exact("hbck,hbsk->hbcs", readout_scaled, removal_back) * closed
    reach_write = einsum_exact("hbck,hbsk->hbcs", readout_scaled, written_back) * closed
    inverse = jnp.eye(BLOCK, dtype=jnp.float32) + lower
    power = lower
    for doubling in range(BLOCK.bit_length() - 2):
        power = einsum_exact("hbcs,hbst->hbct", power, power)
        inverse = inverse + einsum_exact("hbcs,hbst->hbct", inverse, power)
    solved_probe = einsum_exact("hbcs,hbsk->hbck", inverse, probe)
    solved_values = einsum_exact(
        "hbcs,hbsv->hbcv", inverse, einsum_exact("hbcs,hbsv->hbcv", lower_write, value_rows)
    )
    transition = jnp.exp(block_total[:, :, 0, :])[..., None] * jnp.eye(
        HD, dtype=jnp.float32
    ) + einsum_exact("hbck,hbcj->hbkj", removal_tail, solved_probe)
    increment = einsum_exact("hbck,hbcv->hbkv", removal_tail, solved_values) + einsum_exact(
        "hbck,hbcv->hbkv", written_tail, value_rows
    )
    read_state = readout_scaled + einsum_exact("hbcs,hbsk->hbck", reach, solved_probe)
    local_out = einsum_exact("hbcs,hbsv->hbcv", reach, solved_values) + einsum_exact(
        "hbcs,hbsv->hbcv", reach_write, value_rows
    )
    return (transition, increment, read_state, local_out)


def entering(transition, increment):
    peers, position = (lax.axis_size(EP), lax.axis_index(EP))
    zero = jnp.zeros_like(transition)
    identity = jnp.broadcast_to(jnp.eye(HD, dtype=jnp.float32), transition.shape)
    inclusive = jnp.concatenate([transition, increment], axis=-1)
    exclusive = jnp.concatenate([identity, zero], axis=-1)

    def after(preceding, following):
        moved = einsum_exact("quc,qcd->qud", following[..., :HD], preceding)
        return moved + jnp.concatenate([zero, following[..., HD:]], axis=-1)

    shift = 1
    while shift < peers:
        pairs = [(i, i + shift) for i in range(peers - shift)]
        came = lax.ppermute(inclusive.astype(jnp.bfloat16), EP, pairs).astype(jnp.float32)
        later = position >= shift
        exclusive = jnp.where(later, after(came, exclusive), exclusive)
        inclusive = jnp.where(later, after(came, inclusive), inclusive)
        shift *= 2
    return exclusive[..., HD:]


def mixer_half(receptance, key_in, value_in, decay_in, rate_in, norm_gain, out_weight):
    transition, increment, read_state, local_out = block_tables(
        receptance, key_in, value_in, decay_in, rate_in
    )
    head_count, block_count = transition.shape[:2]
    device_map = transition[:, 0]
    device_add = increment[:, 0]
    for k in range(1, block_count):
        step = transition[:, k]
        device_map = einsum_exact("quc,qcd->qud", step, device_map)
        device_add = einsum_exact("quc,qcd->qud", step, device_add) + increment[:, k]
    state = entering(device_map, device_add)
    entries = []
    for k in range(block_count):
        entries.append(state)
        if k + 1 < block_count:
            state = einsum_exact("quc,qcd->qud", transition[:, k], state) + increment[:, k]
    entry_state = jnp.stack(entries, axis=1)
    heads_out = einsum_exact("hbck,hbkv->hbcv", read_state, entry_state) + local_out
    center = heads_out - jnp.mean(heads_out, axis=-1, keepdims=True)
    spread = jnp.mean(center * center, axis=-1, keepdims=True)
    normed = center * lax.rsqrt(spread + 1.0) * norm_gain.reshape(head_count, 1, 1, HD)
    mixed = normed.transpose(1, 2, 0, 3).reshape(receptance.shape).astype(jnp.bfloat16)
    product = jnp.dot(mixed, out_weight, preferred_element_type=jnp.float32).astype(jnp.bfloat16)
    peers = lax.axis_size(TP)
    tiles = exchanged(product.reshape(peers, product.shape[0] // peers, -1), TP)
    return jnp.sum(tiles.astype(jnp.float32), axis=0).astype(jnp.bfloat16)


def expert_half(moe_in, ffn_gain, routes, route_weights, gate_weight, up_weight, down_weight):
    rows, features = moe_in.shape
    tp = lax.axis_size(TP)
    width = features // tp
    at = lax.axis_index(TP) * width
    both = jnp.concatenate([gate_weight[0], up_weight[0]], axis=1)
    side = lax.axis_size("tp_y")
    weights = exchanged(both.reshape(side, features // side, -1), "tp_y")
    total = EXPERTS * SLOT
    f32 = jnp.float32
    outgoing, rank, share = call(
        prep_kernel,
        (
            jax.ShapeDtypeStruct((total, 128), jnp.bfloat16),
            jax.ShapeDtypeStruct((rows, EXPERTS), f32),
            jax.ShapeDtypeStruct((rows, EXPERTS), f32),
        ),
        moe_in,
        lax.dynamic_slice_in_dim(moe_in, at, width, 1),
        lax.dynamic_slice_in_dim(ffn_gain, at, width, 0).reshape(1, width),
        routes,
        route_weights,
    )
    arrived = exchanged(outgoing.reshape(EXPERTS, SLOT, 128), EP).reshape(total, 128)
    gathered = sent_to_all(arrived, "tp_x")
    share_rows = EXPERTS * CAP // side
    wide = weights.shape[0] * weights.shape[2]
    partial = call(
        gate_up_kernel, jax.ShapeDtypeStruct((side, share_rows, wide), jnp.bfloat16), gathered, weights
    )
    parts = exchanged(partial, "tp_y")
    hidden = call(hidden_kernel, jax.ShapeDtypeStruct((share_rows, wide // 2), jnp.bfloat16), parts)
    everyone = sent_to_all(hidden, TP)
    result = call(
        down_kernel, jax.ShapeDtypeStruct((total, 128), jnp.bfloat16), everyone, down_weight[0]
    )
    returned = exchanged(result.reshape(EXPERTS, SLOT, 128), EP).reshape(total, 128)
    return call(
        combine_kernel, jax.ShapeDtypeStruct((rows, width), jnp.bfloat16), returned, rank, share
    )


def local(
    receptance,
    key_in,
    value_in,
    decay_in,
    rate_in,
    norm_gain,
    out_weight,
    moe_in,
    ffn_gain,
    routes,
    route_weights,
    gate_weight,
    up_weight,
    down_weight,
):
    moe_out = expert_half(
        moe_in, ffn_gain, routes, route_weights, gate_weight, up_weight, down_weight
    )
    mixer_out = mixer_half(receptance, key_in, value_in, decay_in, rate_in, norm_gain, out_weight)
    return (mixer_out, moe_out)


def solution(mesh):
    finer = Mesh(mesh.devices.reshape(16, 2, 4, 4), EP_TP)
    placed = (
        P(EP, TP),
        P(EP, TP),
        P(EP, TP),
        P(EP, TP),
        P(EP, TP),
        P(TP),
        P(TP, None),
        P(EP, None),
        P(),
        P(EP, None),
        P(EP, None),
        P(EP, None, TP),
        P(EP, None, TP),
        P(EP, None, TP),
    )
    return jax.shard_map(
        local, mesh=finer, in_specs=placed, out_specs=(P(EP_TP, None), P(EP, TP)), check_vma=False
    )
```

```python
import jax
import jax.numpy as jnp
from jax import lax
from jax.experimental import pallas as pl
from jax.experimental.pallas import tpu as pltpu
from jax.sharding import Mesh
from jax.sharding import PartitionSpec as P

HD = 64
BLOCK = 64
EP = ("ep_0", "ep_1")
TP = ("tp_y", "tp_x")
EP_TP = ("ep_0", "ep_1", "tp_y", "tp_x")
EXPERTS = 32
CAP = 20
SLOT = 2 * CAP
GROUP = 8


def iota(shape, dim):
    return lax.broadcasted_iota(jnp.int32, shape, dim)


def nt(a, b):
    return lax.dot_general(a, b, (((1,), (1,)), ((), ())), preferred_element_type=jnp.float32)


def mm(a, b):
    return jnp.dot(a, b, preferred_element_type=jnp.float32)


NN = (((1,), (0,)), ((), ()))
NT = (((1,), (1,)), ((), ()))
TN = (((0,), (0,)), ((), ()))


def halves(a):
    high = a.astype(jnp.bfloat16)
    return high, (a - high.astype(jnp.float32)).astype(jnp.bfloat16)


def dot(a, b, dims):
    return lax.dot_general(a, b, dims, preferred_element_type=jnp.float32)


def fine_dot(a, b, dims=NN):
    ah, al = halves(a)
    bh, bl = halves(b)
    return dot(ah, bh, dims) + dot(ah, bl, dims) + dot(al, bh, dims)


def call(kernel, outs, *args, scalars=0, scratch=()):
    whole = [pl.BlockSpec(memory_space=pltpu.VMEM)] * (len(args) - scalars)
    return pl.pallas_call(
        kernel,
        out_shape=outs,
        in_specs=[pl.BlockSpec(memory_space=pltpu.SMEM)] * scalars + whole,
        scratch_shapes=list(scratch),
    )(*args)


def shape(dims, dtype=jnp.bfloat16):
    return jax.ShapeDtypeStruct(dims, dtype)


def prep_kernel(place, x, gain, routes, weights, out, rank_out, share_out):
    rows = x.shape[0]
    full = x[...].astype(jnp.float32)
    scale = lax.rsqrt(jnp.mean(full * full, axis=-1, keepdims=True) + 1.0)
    mine = pl.ds(pl.multiple_of(place[0] * 256, 256), 256)
    piece = (x[:, mine].astype(jnp.float32) * scale * gain[:, mine]).astype(jnp.bfloat16)
    w = weights[...]
    portion = w / jnp.sum(w, axis=0, keepdims=True)
    expert = iota((EXPERTS, rows), 0)
    chosen = jnp.zeros((EXPERTS, rows), jnp.float32)
    share = jnp.zeros((EXPERTS, rows), jnp.float32)
    for j in range(routes.shape[0]):
        hit = routes[j : j + 1, :] == expert
        chosen = jnp.where(hit, 1.0, chosen)
        share = jnp.where(hit, portion[j : j + 1, :], share)
    earlier = (iota((rows, rows), 0) <= iota((rows, rows), 1)).astype(jnp.bfloat16)
    rank = mm(chosen.astype(jnp.bfloat16), earlier) * chosen
    rank_out[...] = rank
    share_out[...] = share
    total = EXPERTS * SLOT
    q = iota((total, EXPERTS), 0)
    spread = (q // SLOT == iota((total, EXPERTS), 1)).astype(jnp.bfloat16)
    seat = (iota((total, rows), 0) % CAP + 1).astype(jnp.float32)
    pick = (mm(spread, rank.astype(jnp.bfloat16)) == seat).astype(jnp.bfloat16)
    both = mm(pick, piece)
    second = iota((total, 128), 0) % SLOT >= CAP
    out[...] = jnp.where(second, both[:, 128:], both[:, :128]).astype(jnp.bfloat16)


def combine_kernel(back, rank, share, out):
    rows = rank.shape[1]
    total = EXPERTS * SLOT
    rank = jnp.transpose(rank[...])
    share = jnp.transpose(share[...])
    spread = (iota((total, EXPERTS), 0) // SLOT == iota((total, EXPERTS), 1)).astype(jnp.bfloat16)
    q = iota((rows, total), 1)
    match = nt(rank.astype(jnp.bfloat16), spread) == (q % CAP + 1).astype(jnp.float32)
    second = q % SLOT >= CAP
    high, low = halves(share)
    values = back[...]
    first_half = jnp.zeros((rows, 128), jnp.float32)
    second_half = jnp.zeros((rows, 128), jnp.float32)
    for part in (high, low):
        wide = jnp.where(match, nt(part, spread), 0.0)
        first_half += mm(jnp.where(second, 0.0, wide).astype(jnp.bfloat16), values)
        second_half += mm(jnp.where(second, wide, 0.0).astype(jnp.bfloat16), values)
    out[:, :128] = first_half.astype(out.dtype)
    out[:, 128:] = second_half.astype(out.dtype)


def selector(half):
    r = iota((GROUP * CAP, GROUP * SLOT), 0)
    return (iota((GROUP * CAP, GROUP * SLOT), 1) == r // CAP * SLOT + r % CAP + half * CAP).astype(
        jnp.bfloat16
    )


def gate_up_kernel(place, gathered, w0, w1, w2, w3, out, weights):
    picks = (selector(0), selector(1))
    side = weights.shape[0]
    for back, w in enumerate((w0, w1, w2, w3)):
        weights[(place[0] + side - back) % side] = w[: weights.shape[1], :]
    joined = jnp.concatenate([weights[k] for k in range(side)], axis=1)
    for g in range(EXPERTS // GROUP):
        pieces = []
        for k in range(gathered.shape[0]):
            seen = gathered[k, g * GROUP * SLOT : (g + 1) * GROUP * SLOT, :]
            for pick in picks:
                pieces.append(mm(pick, seen).astype(jnp.bfloat16))
        out[g] = mm(jnp.concatenate(pieces, axis=1), joined).astype(jnp.bfloat16)


def hidden_kernel(parts, out):
    both = jnp.zeros(parts.shape[1:], jnp.float32)
    for k in range(parts.shape[0]):
        both += parts[k].astype(jnp.float32)
    made = []
    for k in range(both.shape[1] // 128):
        v = both[:, k * 128 : (k + 1) * 128]
        made.append(jax.nn.silu(v) * pltpu.roll(v, 64, 1))
    left = iota((both.shape[0], 128), 1) < 64
    for k in range(len(made) // 2):
        value = jnp.where(left, made[2 * k], pltpu.roll(made[2 * k + 1], 64, 1))
        for peer in range(out.shape[0]):
            out[peer, :, k * 128 : (k + 1) * 128] = value.astype(jnp.bfloat16)


def down_kernel(hidden, weights, out):
    picks = (selector(0), selector(1))
    side = 4
    tall = []
    for k in range(side):
        tall.append(
            jnp.concatenate(
                [weights[(side * m + k) * 64 : (side * m + k + 1) * 64, :] for m in range(side)], 0
            )
        )
    for g in range(side):
        total = mm(hidden[side * g], tall[0])
        for k in range(1, side):
            total += mm(hidden[side * g + k], tall[k])
        total = total.astype(jnp.bfloat16)
        placed = jnp.zeros((GROUP * SLOT, 128), jnp.float32)
        for half in range(2):
            placed += lax.dot_general(
                picks[half],
                total[:, half * 128 : (half + 1) * 128],
                (((0,), (0,)), ((), ())),
                preferred_element_type=jnp.float32,
            )
        out[g * GROUP * SLOT : (g + 1) * GROUP * SLOT, :] = placed.astype(jnp.bfloat16)


def exchanged(tiles, axis):
    return lax.all_to_all(tiles, axis, split_axis=0, concat_axis=0, tiled=True)


def sent_to_all(shard, axis):
    return exchanged(jnp.broadcast_to(shard, (lax.axis_size(axis), *shard.shape)), axis)


def head_sums(a):
    left = iota(a.shape, 1) < HD
    low = jnp.sum(jnp.where(left, a, 0.0), axis=-1, keepdims=True)
    high = jnp.sum(jnp.where(left, 0.0, a), axis=-1, keepdims=True)
    return jnp.where(left, low, high)


def tables_kernel(receptance, key_in, value_in, decay_in, rate_in, inc, inc_send, read, local_out):
    f32 = jnp.float32
    size = (BLOCK, BLOCK)
    strict = (iota(size, 1) < iota(size, 0)).astype(f32)
    closed = (iota(size, 1) <= iota(size, 0)).astype(f32)
    eye = (iota(size, 1) == iota(size, 0)).astype(f32)
    summing = closed.astype(jnp.bfloat16)
    count = receptance.shape[0] // BLOCK
    heads = receptance.shape[1] // HD
    state = [jnp.concatenate([eye, jnp.zeros(size, f32)], axis=1) for _ in range(heads)]
    blocks = []
    for b in range(count):
        at = slice(b * BLOCK, (b + 1) * BLOCK)
        readout = receptance[at, :].astype(f32)
        key = key_in[at, :].astype(f32)
        value = value_in[at, :].astype(f32)
        log_decay = -jnp.exp(-jax.nn.softplus(-decay_in[at, :].astype(f32)) - 0.5)
        rate = jax.nn.sigmoid(rate_in[at, :].astype(f32))
        unit = key / jnp.sqrt(head_sums(key * key) + 1.0)
        first, _ = halves(log_decay)
        middle = (log_decay - first.astype(f32)).astype(jnp.bfloat16)
        last = (log_decay - first.astype(f32) - middle.astype(f32)).astype(jnp.bfloat16)
        inclusive = mm(summing, first) + mm(summing, middle) + mm(summing, last)
        total = inclusive[BLOCK - 1 :, :]
        probe = -unit * jnp.exp(inclusive - log_decay)
        removal = unit * rate
        written = key * rate
        grow = jnp.exp(-inclusive)
        tail = jnp.exp(total - inclusive)
        blocks.append(
            (
                probe,
                readout * jnp.exp(inclusive),
                removal * grow,
                written * grow,
                removal * tail,
                written * tail,
                value,
                jnp.exp(total),
            )
        )
    work = []
    for b in range(count):
        for h in range(heads):
            side = slice(h * HD, (h + 1) * HD)
            cut = [a[:, side] for a in blocks[b]]
            probe, readout, removal, written, removal_tail, written_tail, value, total = cut
            meet = fine_dot(
                jnp.concatenate([probe, readout], 0), jnp.concatenate([removal, written], 0), NT
            )
            work.append(
                dict(
                    lower=meet[:BLOCK, :BLOCK] * strict,
                    write=meet[:BLOCK, BLOCK:] * strict,
                    reach=meet[BLOCK:, :BLOCK] * closed,
                    reach_write=meet[BLOCK:, BLOCK:] * closed,
                    probe=probe,
                    readout=readout,
                    removal_tail=removal_tail,
                    written_tail=written_tail,
                    value=value,
                    total=total,
                )
            )
    inverses = [eye + w["lower"] for w in work]
    powers = [fine_dot(w["lower"], w["lower"]) for w in work]
    for step in range(BLOCK.bit_length() - 2):
        for k in range(len(work)):
            if step + 3 < BLOCK.bit_length():
                both = fine_dot(jnp.concatenate([inverses[k], powers[k]], 0), powers[k])
                inverses[k] = inverses[k] + both[:BLOCK]
                powers[k] = both[BLOCK:]
            else:
                inverses[k] = inverses[k] + fine_dot(inverses[k], powers[k])
    zero = jnp.zeros(size, f32)
    steps = []
    for k, w in enumerate(work):
        seen = fine_dot(w["write"], w["value"])
        solved = fine_dot(inverses[k], jnp.concatenate([w["probe"], seen], 1))
        right = jnp.concatenate([solved, jnp.concatenate([zero, w["value"]], 1)], 0)
        moved = fine_dot(jnp.concatenate([w["removal_tail"], w["written_tail"]], 0), right, TN)
        heard = fine_dot(jnp.concatenate([w["reach"], w["reach_write"]], 1), right)
        steps.append(
            (
                jnp.concatenate([w["readout"] + heard[:, :HD], eye * w["total"] + moved[:, :HD]], 0),
                jnp.concatenate([heard[:, HD:], moved[:, HD:]], 0),
            )
        )
    for b in range(count):
        at = slice(b * BLOCK, (b + 1) * BLOCK)
        reads = []
        locals_ = []
        for h in range(heads):
            maps, adds = steps[b * heads + h]
            new = fine_dot(maps, state[h])
            added = new[:, HD:] + adds
            reads.append(new[:BLOCK, :HD])
            locals_.append(added[:BLOCK])
            state[h] = jnp.concatenate([new[BLOCK:, :HD], added[BLOCK:]], 1)
        read[at, :] = jnp.concatenate(reads, 1)
        local_out[at, :] = jnp.concatenate(locals_, 1)
    for h in range(heads):
        inc[h] = state[h]
        inc_send[h] = state[h].astype(jnp.bfloat16)


def round_kernel(later, came, inc, exc, inc_out, exc_out, send_out):
    heads, rows, lanes = inc.shape
    go = later[0] > 0
    right = iota((2 * rows, lanes), 1) >= HD
    for h in range(heads):
        old = jnp.concatenate([inc[h], exc[h]], 0)
        high, low = halves(old[:, :HD])
        new = mm(high, came[h]) + mm(low, came[h]) + jnp.where(right, old, 0.0)
        new = jnp.where(go, new, old)
        inc_out[h] = new[:rows]
        exc_out[h] = new[rows:]
        send_out[h] = new[:rows].astype(jnp.bfloat16)


def readout_kernel(read, local_out, exc, gain, out):
    first = exc[0][:, HD:]
    second = exc[1][:, HD:]
    zero = jnp.zeros_like(first)
    state = jnp.concatenate(
        [jnp.concatenate([first, zero], 1), jnp.concatenate([zero, second], 1)], 0
    )
    seen = fine_dot(read[...], state) + local_out[...]
    center = seen - head_sums(seen) / HD
    spread = head_sums(center * center) / HD
    out[...] = (center * lax.rsqrt(spread + 1.0) * gain[...]).astype(jnp.bfloat16)


def pack_kernel(place, gate, up, out_weight, p0, p1, p2, p3):
    side = 4
    length = gate.shape[0] // side
    for ahead, p in enumerate((p0, p1, p2, p3)):
        target = (place[0] + ahead) % side
        at = pl.ds(pl.multiple_of(target * length, length), length)
        p[:length, :] = jnp.concatenate([gate[at, :], up[at, :]], axis=1)
        for c in range(length // 128):
            tile = pl.ds(pl.multiple_of(target * length + c * 128, 128), 128)
            p[length + c * 128 : length + (c + 1) * 128, :] = out_weight[:, tile]


def product_kernel(m0, m1, m2, m3, w0, w1, w2, w3, out):
    rows = jnp.concatenate([m[...] for m in (m0, m1, m2, m3)], 1)
    peers, each, columns = out.shape
    top = w0.shape[0] - columns
    for c in range(columns // 256):
        tiles = []
        for w in (w0, w1, w2, w3):
            low = top + c * 256
            tiles.append(jnp.concatenate([w[low : low + 128, :], w[low + 128 : low + 256, :]], 1))
        made = mm(rows, jnp.concatenate(tiles, 0)).astype(jnp.bfloat16)
        for p in range(peers):
            out[p, :, c * 256 : (c + 1) * 256] = made[p * each : (p + 1) * each]


def finish_kernel(tiles, out):
    side = 4
    width = tiles.shape[2]
    for y in range(side):
        total = tiles[side * y].astype(jnp.float32)
        for x in range(1, side):
            total += tiles[side * y + x].astype(jnp.float32)
        out[:, y * width : (y + 1) * width] = total.astype(jnp.bfloat16)


def turned(shard, axis, back):
    n = lax.axis_size(axis)
    return lax.ppermute(shard, axis, [(i, (i + back) % n) for i in range(n)])


def local(
    receptance,
    key_in,
    value_in,
    decay_in,
    rate_in,
    norm_gain,
    out_weight,
    moe_in,
    ffn_gain,
    routes,
    route_weights,
    gate_weight,
    up_weight,
    down_weight,
):
    f32 = jnp.float32
    rows, features = moe_in.shape
    tp = lax.axis_size(TP)
    side = lax.axis_size("tp_y")
    width = features // tp
    row_place = lax.axis_index("tp_y").astype(jnp.int32).reshape(1)
    total = EXPERTS * SLOT
    share_rows = EXPERTS * CAP // side
    outgoing, rank, share = call(
        prep_kernel,
        (shape((total, 128)), shape((EXPERTS, rows), f32), shape((EXPERTS, rows), f32)),
        lax.axis_index(TP).astype(jnp.int32).reshape(1),
        moe_in,
        ffn_gain.reshape(1, features),
        routes.T,
        route_weights.T,
        scalars=1,
    )
    arrived = exchanged(outgoing.reshape(EXPERTS, SLOT, 128), EP)
    packs = call(
        pack_kernel,
        [shape((2 * features // side, 128))] * side,
        row_place,
        gate_weight[0],
        up_weight[0],
        out_weight,
        scalars=1,
    )
    moved = [packs[0]] + [turned(packs[k], "tp_y", k) for k in range(1, side)]

    tokens, columns = receptance.shape
    heads = columns // HD
    pack = (heads, HD, 2 * HD)
    inc, send, read, local_out = call(
        tables_kernel,
        (shape(pack, f32), shape(pack), shape((tokens, columns), f32), shape((tokens, columns), f32)),
        receptance,
        key_in,
        value_in,
        decay_in,
        rate_in,
    )
    eye = jnp.concatenate([jnp.eye(HD, dtype=f32), jnp.zeros((HD, HD), f32)], 1)
    exc = jnp.broadcast_to(eye, pack)
    peers, position = (lax.axis_size(EP), lax.axis_index(EP))
    shift = 1
    while shift < peers:
        came = lax.ppermute(send, EP, [(i, i + shift) for i in range(peers - shift)])
        inc, exc, send = call(
            round_kernel,
            (shape(pack, f32), shape(pack, f32), shape(pack)),
            (position >= shift).astype(jnp.int32).reshape(1),
            came,
            inc,
            exc,
            scalars=1,
        )
        shift = 2 * shift
    mixed = call(
        readout_kernel,
        shape((tokens, columns)),
        read,
        local_out,
        exc,
        norm_gain.reshape(1, columns),
    )
    mixes = [mixed] + [turned(mixed, "tp_y", k) for k in range(1, side)]
    product = call(
        product_kernel, shape((tp, tokens // tp, features // side)), *mixes, *moved
    )

    gathered = sent_to_all(arrived.reshape(total, 128), "tp_x")
    wide = side * 128
    partial = call(
        gate_up_kernel,
        shape((side, share_rows, wide)),
        row_place,
        gathered,
        *moved,
        scalars=1,
        scratch=[pltpu.VMEM((side, features // side, 128), jnp.bfloat16)],
    )
    parts = exchanged(partial, "tp_y")
    hidden = call(hidden_kernel, shape((tp, share_rows, wide // 2)), parts)
    everyone = exchanged(hidden, TP)
    result = call(down_kernel, shape((total, 128)), everyone, down_weight[0])
    returned = exchanged(result.reshape(EXPERTS, SLOT, 128), EP)
    tiles = exchanged(product, TP)
    moe_out = call(combine_kernel, shape((rows, width)), returned.reshape(total, 128), rank, share)
    mixer_out = call(
        finish_kernel, shape((tokens // tp, side * product.shape[2])), tiles
    )
    return (mixer_out, moe_out)


def solution(mesh):
    finer = Mesh(mesh.devices.reshape(16, 2, 4, 4), EP_TP)
    placed = (
        P(EP, TP),
        P(EP, TP),
        P(EP, TP),
        P(EP, TP),
        P(EP, TP),
        P(TP),
        P(TP, None),
        P(EP, None),
        P(),
        P(EP, None),
        P(EP, None),
        P(EP, None, TP),
        P(EP, None, TP),
        P(EP, None, TP),
    )
    return jax.shard_map(
        local, mesh=finer, in_specs=placed, out_specs=(P(EP_TP, None), P(EP, TP)), check_vma=False
    )
```

```python
import functools

import jax
import jax.numpy as jnp
from jax import lax
from jax.experimental import pallas as pl
from jax.experimental.pallas import tpu as pltpu
from jax.sharding import Mesh
from jax.sharding import PartitionSpec as P

HD = 64
BLOCK = 64
EP = ("ep_0", "ep_1")
TP = ("tp_y", "tp_x")
EP_TP = ("ep_0", "ep_1", "tp_y", "tp_x")
EXPERTS = 32
CAP = 20
SLOT = 2 * CAP
GROUP = 8
LIMIT = 16 * 1024 * 1024


def iota(shape, dim):
    return lax.broadcasted_iota(jnp.int32, shape, dim)


def nt(a, b):
    return lax.dot_general(a, b, (((1,), (1,)), ((), ())), preferred_element_type=jnp.float32)


def mm(a, b):
    return jnp.dot(a, b, preferred_element_type=jnp.float32)


NN = (((1,), (0,)), ((), ()))
NT = (((1,), (1,)), ((), ()))
TN = (((0,), (0,)), ((), ()))


def halves(a):
    high = a.astype(jnp.bfloat16)
    return high, (a - high.astype(jnp.float32)).astype(jnp.bfloat16)


def dot(a, b, dims):
    return lax.dot_general(a, b, dims, preferred_element_type=jnp.float32)


def fine_dot(a, b, dims=NN):
    ah, al = halves(a)
    bh, bl = halves(b)
    return dot(ah, bh, dims) + dot(ah, bl, dims) + dot(al, bh, dims)


def call(kernel, outs, *args, scalars=0, scratch=(), limit=LIMIT):
    whole = [pl.BlockSpec(memory_space=pltpu.VMEM)] * (len(args) - scalars)
    return pl.pallas_call(
        kernel,
        out_shape=outs,
        in_specs=[pl.BlockSpec(memory_space=pltpu.SMEM)] * scalars + whole,
        scratch_shapes=list(scratch),
        compiler_params=pltpu.CompilerParams(vmem_limit_bytes=limit),
    )(*args)


def shape(dims, dtype=jnp.bfloat16):
    return jax.ShapeDtypeStruct(dims, dtype)


def prep_kernel(place, x, gain, routes, weights, out, rank_out, share_out):
    rows = x.shape[0]
    full = x[...].astype(jnp.float32)
    scale = lax.rsqrt(jnp.mean(full * full, axis=-1, keepdims=True) + 1.0)
    mine = pl.ds(pl.multiple_of(place[0] * 256, 256), 256)
    piece = (x[:, mine].astype(jnp.float32) * scale * gain[:, mine]).astype(jnp.bfloat16)
    w = weights[...]
    portion = w / jnp.sum(w, axis=0, keepdims=True)
    expert = iota((EXPERTS, rows), 0)
    chosen = jnp.zeros((EXPERTS, rows), jnp.float32)
    share = jnp.zeros((EXPERTS, rows), jnp.float32)
    for j in range(routes.shape[0]):
        hit = routes[j : j + 1, :] == expert
        chosen = jnp.where(hit, 1.0, chosen)
        share = jnp.where(hit, portion[j : j + 1, :], share)
    earlier = (iota((rows, rows), 0) <= iota((rows, rows), 1)).astype(jnp.bfloat16)
    rank = mm(chosen.astype(jnp.bfloat16), earlier) * chosen
    rank_out[...] = rank
    share_out[...] = share
    total = EXPERTS * SLOT
    q = iota((total, EXPERTS), 0)
    spread = (q // SLOT == iota((total, EXPERTS), 1)).astype(jnp.bfloat16)
    seat = (iota((total, rows), 0) % CAP + 1).astype(jnp.float32)
    pick = (mm(spread, rank.astype(jnp.bfloat16)) == seat).astype(jnp.bfloat16)
    both = mm(pick, piece)
    second = iota((total, 128), 0) % SLOT >= CAP
    out[...] = jnp.where(second, both[:, 128:], both[:, :128]).astype(jnp.bfloat16)


def combine_kernel(back, rank, share, out):
    rows = rank.shape[1]
    total = EXPERTS * SLOT
    rank = jnp.transpose(rank[...])
    share = jnp.transpose(share[...])
    spread = (iota((total, EXPERTS), 0) // SLOT == iota((total, EXPERTS), 1)).astype(jnp.bfloat16)
    q = iota((rows, total), 1)
    match = nt(rank.astype(jnp.bfloat16), spread) == (q % CAP + 1).astype(jnp.float32)
    second = q % SLOT >= CAP
    high, low = halves(share)
    values = back[...]
    first_half = jnp.zeros((rows, 128), jnp.float32)
    second_half = jnp.zeros((rows, 128), jnp.float32)
    for part in (high, low):
        wide = jnp.where(match, nt(part, spread), 0.0)
        first_half += mm(jnp.where(second, 0.0, wide).astype(jnp.bfloat16), values)
        second_half += mm(jnp.where(second, wide, 0.0).astype(jnp.bfloat16), values)
    out[:, :128] = first_half.astype(out.dtype)
    out[:, 128:] = second_half.astype(out.dtype)


def selector(half):
    r = iota((GROUP * CAP, GROUP * SLOT), 0)
    return (iota((GROUP * CAP, GROUP * SLOT), 1) == r // CAP * SLOT + r % CAP + half * CAP).astype(
        jnp.bfloat16
    )


def gate_up_kernel(place, gathered, w0, w1, w2, w3, out, weights):
    picks = (selector(0), selector(1))
    side = weights.shape[0]
    for back, w in enumerate((w0, w1, w2, w3)):
        weights[(place[0] + side - back) % side] = w[: weights.shape[1], :]
    joined = jnp.concatenate([weights[k] for k in range(side)], axis=0)
    for g in range(EXPERTS // GROUP):
        pieces = []
        for k in range(gathered.shape[0]):
            seen = gathered[k, g * GROUP * SLOT : (g + 1) * GROUP * SLOT, :]
            for pick in picks:
                pieces.append(mm(pick, seen).astype(jnp.bfloat16))
        out[g] = nt(jnp.concatenate(pieces, axis=1), joined).astype(jnp.bfloat16)


def hidden_kernel(parts, out):
    both = jnp.zeros(parts.shape[1:], jnp.float32)
    for k in range(parts.shape[0]):
        both += parts[k].astype(jnp.float32)
    made = []
    for k in range(both.shape[1] // 128):
        v = both[:, k * 128 : (k + 1) * 128]
        made.append(jax.nn.silu(v) * pltpu.roll(v, 64, 1))
    left = iota((both.shape[0], 128), 1) < 64
    for k in range(len(made) // 2):
        value = jnp.where(left, made[2 * k], pltpu.roll(made[2 * k + 1], 64, 1))
        for peer in range(out.shape[0]):
            out[peer, :, k * 128 : (k + 1) * 128] = value.astype(jnp.bfloat16)


def down_kernel(hidden, weights, out):
    picks = (selector(0), selector(1))
    side = 4
    tall = []
    for k in range(side):
        tall.append(
            jnp.concatenate(
                [weights[(side * m + k) * 64 : (side * m + k + 1) * 64, :] for m in range(side)], 0
            )
        )
    for g in range(side):
        total = mm(hidden[side * g], tall[0])
        for k in range(1, side):
            total += mm(hidden[side * g + k], tall[k])
        total = total.astype(jnp.bfloat16)
        placed = jnp.zeros((GROUP * SLOT, 128), jnp.float32)
        for half in range(2):
            placed += lax.dot_general(
                picks[half],
                total[:, half * 128 : (half + 1) * 128],
                (((0,), (0,)), ((), ())),
                preferred_element_type=jnp.float32,
            )
        out[g * GROUP * SLOT : (g + 1) * GROUP * SLOT, :] = placed.astype(jnp.bfloat16)


def exchanged(tiles, axis):
    return lax.all_to_all(tiles, axis, split_axis=0, concat_axis=0, tiled=True)


def head_sums(a):
    left = iota(a.shape, 1) < HD
    low = jnp.sum(jnp.where(left, a, 0.0), axis=-1, keepdims=True)
    high = jnp.sum(jnp.where(left, 0.0, a), axis=-1, keepdims=True)
    return jnp.where(left, low, high)


def tables_kernel(receptance, key_in, value_in, decay_in, rate_in, begun, send, table):
    f32 = jnp.float32
    size = (BLOCK, BLOCK)
    strict = (iota(size, 1) < iota(size, 0)).astype(f32)
    closed = (iota(size, 1) <= iota(size, 0)).astype(f32)
    eye = (iota(size, 1) == iota(size, 0)).astype(f32)
    summing = closed.astype(jnp.bfloat16)
    count = receptance.shape[0] // BLOCK
    heads = receptance.shape[1] // HD
    state = [jnp.concatenate([eye, jnp.zeros(size, f32)], axis=1) for _ in range(heads)]
    blocks = []
    for b in range(count):
        at = slice(b * BLOCK, (b + 1) * BLOCK)
        readout = receptance[at, :].astype(f32)
        key = key_in[at, :].astype(f32)
        value = value_in[at, :].astype(f32)
        log_decay = -jnp.exp(-jax.nn.softplus(-decay_in[at, :].astype(f32)) - 0.5)
        rate = jax.nn.sigmoid(rate_in[at, :].astype(f32))
        unit = key / jnp.sqrt(head_sums(key * key) + 1.0)
        first, _ = halves(log_decay)
        middle = (log_decay - first.astype(f32)).astype(jnp.bfloat16)
        last = (log_decay - first.astype(f32) - middle.astype(f32)).astype(jnp.bfloat16)
        inclusive = mm(summing, first) + mm(summing, middle) + mm(summing, last)
        total = inclusive[BLOCK - 1 :, :]
        probe = -unit * jnp.exp(inclusive - log_decay)
        removal = unit * rate
        written = key * rate
        grow = jnp.exp(-inclusive)
        tail = jnp.exp(total - inclusive)
        blocks.append(
            (
                probe,
                readout * jnp.exp(inclusive),
                removal * grow,
                written * grow,
                removal * tail,
                written * tail,
                value,
                jnp.exp(total),
            )
        )
    work = []
    for b in range(count):
        for h in range(heads):
            side = slice(h * HD, (h + 1) * HD)
            cut = [a[:, side] for a in blocks[b]]
            probe, readout, removal, written, removal_tail, written_tail, value, total = cut
            meet = fine_dot(
                jnp.concatenate([probe, readout], 0), jnp.concatenate([removal, written], 0), NT
            )
            work.append(
                dict(
                    lower=meet[:BLOCK, :BLOCK] * strict,
                    write=meet[:BLOCK, BLOCK:] * strict,
                    reach=meet[BLOCK:, :BLOCK] * closed,
                    reach_write=meet[BLOCK:, BLOCK:] * closed,
                    probe=probe,
                    readout=readout,
                    removal_tail=removal_tail,
                    written_tail=written_tail,
                    value=value,
                    total=total,
                )
            )
    inverses = [eye + w["lower"] for w in work]
    powers = [fine_dot(w["lower"], w["lower"]) for w in work]
    for step in range(BLOCK.bit_length() - 2):
        for k in range(len(work)):
            if step + 3 < BLOCK.bit_length():
                both = fine_dot(jnp.concatenate([inverses[k], powers[k]], 0), powers[k])
                inverses[k] = inverses[k] + both[:BLOCK]
                powers[k] = both[BLOCK:]
            else:
                inverses[k] = inverses[k] + fine_dot(inverses[k], powers[k])
    zero = jnp.zeros(size, f32)
    steps = []
    for k, w in enumerate(work):
        seen = fine_dot(w["write"], w["value"])
        solved = fine_dot(inverses[k], jnp.concatenate([w["probe"], seen], 1))
        right = jnp.concatenate([solved, jnp.concatenate([zero, w["value"]], 1)], 0)
        moved = fine_dot(jnp.concatenate([w["removal_tail"], w["written_tail"]], 0), right, TN)
        heard = fine_dot(jnp.concatenate([w["reach"], w["reach_write"]], 1), right)
        steps.append(
            (
                jnp.concatenate([w["readout"] + heard[:, :HD], eye * w["total"] + moved[:, :HD]], 0),
                jnp.concatenate([heard[:, HD:], moved[:, HD:]], 0),
            )
        )
    for b in range(count):
        at = slice(b * BLOCK, (b + 1) * BLOCK)
        reads = []
        locals_ = []
        for h in range(heads):
            maps, adds = steps[b * heads + h]
            new = fine_dot(maps, state[h])
            added = new[:, HD:] + adds
            reads.append(new[:BLOCK, :HD])
            locals_.append(added[:BLOCK])
            state[h] = jnp.concatenate([new[BLOCK:, :HD], added[BLOCK:]], 1)
        table[0, at, :] = jnp.concatenate(reads, 1)
        table[1, at, :] = jnp.concatenate(locals_, 1)
    for h in range(heads):
        begun[h, :HD] = state[h]
        begun[h, HD:] = jnp.concatenate([eye, zero], 1)
        send[h] = state[h].astype(jnp.bfloat16)


def advanced(later, came, old):
    right = iota(old.shape, 1) >= HD
    high, low = halves(old[:, :HD])
    new = mm(high, came) + mm(low, came) + jnp.where(right, old, 0.0)
    return jnp.where(later, new, old)


def round_kernel(position, came, state, state_out, send_out, *, shift):
    for h in range(state.shape[0]):
        new = advanced(position[0] >= shift, came[h], state[h])
        state_out[h] = new
        if len(send_out.shape) == 3:
            send_out[h] = new[:HD].astype(jnp.bfloat16)
        else:
            send_out[:, h * HD : (h + 1) * HD] = new[:HD, HD:].astype(jnp.bfloat16)


def readout_kernel(position, came, last, table, gain, out, *, shift):
    later = position[0] >= shift
    states = []
    for h in range(last.shape[0]):
        side = slice(h * HD, (h + 1) * HD)
        old = last[h, HD:, :]
        high, low = halves(old[:, :HD])
        new = mm(high, came[:, side]) + mm(low, came[:, side]) + old[:, HD:]
        states.append(jnp.where(later, new, old[:, HD:]))
    first, second = states
    zero = jnp.zeros_like(first)
    state = jnp.concatenate(
        [jnp.concatenate([first, zero], 1), jnp.concatenate([zero, second], 1)], 0
    )
    seen = fine_dot(table[0], state) + table[1]
    center = seen - head_sums(seen) / HD
    spread = head_sums(center * center) / HD
    out[...] = (center * lax.rsqrt(spread + 1.0) * gain[...]).astype(jnp.bfloat16)


def copies_kernel(one, out):
    for k in range(out.shape[0]):
        out[k] = one[...]


def pack_kernel(place, gate, up, out_weight, p0, p1, p2, p3):
    side = 4
    hidden, features = gate.shape
    length = features // side
    for ahead, p in enumerate((p0, p1, p2, p3)):
        target = (place[0] + ahead) % side
        at = pl.ds(pl.multiple_of(target * length, length), length)
        p[:hidden, :] = gate[:, at]
        p[hidden : 2 * hidden, :] = up[:, at]
        p[2 * hidden :, :] = out_weight[:, at]


def product_kernel(m0, m1, m2, m3, w0, w1, w2, w3, out):
    rows = jnp.concatenate([m[...] for m in (m0, m1, m2, m3)], 1)
    count = rows.shape[1] // 4
    weights = jnp.concatenate([w[w.shape[0] - count :, :] for w in (w0, w1, w2, w3)], 0)
    made = mm(rows, weights).astype(jnp.bfloat16)
    peers, each, _ = out.shape
    for p in range(peers):
        out[p] = made[p * each : (p + 1) * each]


def finish_kernel(tiles, out):
    side = 4
    width = tiles.shape[2]
    for y in range(side):
        total = tiles[side * y].astype(jnp.float32)
        for x in range(1, side):
            total += tiles[side * y + x].astype(jnp.float32)
        out[:, y * width : (y + 1) * width] = total.astype(jnp.bfloat16)


def turned(shard, axis, back):
    n = lax.axis_size(axis)
    return lax.ppermute(shard, axis, [(i, (i + back) % n) for i in range(n)])


def local(
    receptance,
    key_in,
    value_in,
    decay_in,
    rate_in,
    norm_gain,
    out_weight,
    moe_in,
    ffn_gain,
    routes,
    route_weights,
    gate_weight,
    up_weight,
    down_weight,
):
    f32 = jnp.float32
    rows, features = moe_in.shape
    tp = lax.axis_size(TP)
    side = lax.axis_size("tp_y")
    width = features // tp
    row_place = lax.axis_index("tp_y").astype(jnp.int32).reshape(1)
    total = EXPERTS * SLOT
    share_rows = EXPERTS * CAP // side
    outgoing, rank, share = call(
        prep_kernel,
        (shape((total, 128)), shape((EXPERTS, rows), f32), shape((EXPERTS, rows), f32)),
        lax.axis_index(TP).astype(jnp.int32).reshape(1),
        moe_in,
        ffn_gain.reshape(1, features),
        routes.T,
        route_weights.T,
        scalars=1,
        limit=None,
    )
    arrived = exchanged(outgoing.reshape(EXPERTS, SLOT, 128), EP)
    packs = call(
        pack_kernel,
        [shape((256, features // side))] * side,
        row_place,
        gate_weight[0].T,
        up_weight[0].T,
        out_weight,
        scalars=1,
    )
    moved = [packs[0]] + [turned(packs[k], "tp_y", k) for k in range(1, side)]

    tokens, columns = receptance.shape
    heads = columns // HD
    pack = (heads, HD, 2 * HD)
    stack = (heads, 2 * HD, 2 * HD)
    flat = (tokens, columns)
    state, send, table = call(
        tables_kernel,
        (shape(stack, f32), shape(pack), shape((2, *flat), f32)),
        receptance,
        key_in,
        value_in,
        decay_in,
        rate_in,
    )
    peers = lax.axis_size(EP)
    position = lax.axis_index(EP).astype(jnp.int32).reshape(1)
    shift = 1
    while shift < peers:
        came = lax.ppermute(send, EP, [(i, i + shift) for i in range(peers - shift)])
        if 2 * shift < peers:
            state, send = call(
                functools.partial(round_kernel, shift=shift),
                (shape(stack, f32), shape(pack if 4 * shift < peers else (HD, 2 * HD))),
                position,
                came,
                state,
                scalars=1,
            )
        shift = 2 * shift
    mixed = call(
        functools.partial(readout_kernel, shift=shift // 2),
        shape(flat),
        position,
        came,
        state,
        table,
        norm_gain.reshape(1, columns),
        scalars=1,
    )
    mixes = [mixed] + [turned(mixed, "tp_y", k) for k in range(1, side)]
    product = call(
        product_kernel, shape((tp, tokens // tp, features // side)), *mixes, *moved
    )

    copies = call(
        copies_kernel, shape((side, total, 128)), arrived.reshape(total, 128)
    )
    gathered = exchanged(copies, "tp_x")
    wide = side * 128
    partial = call(
        gate_up_kernel,
        shape((side, share_rows, wide)),
        row_place,
        gathered,
        *moved,
        scalars=1,
        scratch=[pltpu.VMEM((side, 128, features // side), jnp.bfloat16)],
    )
    parts = exchanged(partial, "tp_y")
    hidden = call(hidden_kernel, shape((tp, share_rows, wide // 2)), parts)
    everyone = exchanged(hidden, TP)
    result = call(down_kernel, shape((total, 128)), everyone, down_weight[0])
    returned = exchanged(result.reshape(EXPERTS, SLOT, 128), EP)
    tiles = exchanged(product, TP)
    moe_out = call(combine_kernel, shape((rows, width)), returned.reshape(total, 128), rank, share)
    mixer_out = call(
        finish_kernel, shape((tokens // tp, side * product.shape[2])), tiles
    )
    return (mixer_out, moe_out)


def solution(mesh):
    finer = Mesh(mesh.devices.reshape(16, 2, 4, 4), EP_TP)
    placed = (
        P(EP, TP),
        P(EP, TP),
        P(EP, TP),
        P(EP, TP),
        P(EP, TP),
        P(TP),
        P(TP, None),
        P(EP, None),
        P(),
        P(EP, None),
        P(EP, None),
        P(EP, None, TP),
        P(EP, None, TP),
        P(EP, None, TP),
    )
    return jax.shard_map(
        local, mesh=finer, in_specs=placed, out_specs=(P(EP_TP, None), P(EP, TP)), check_vma=False
    )
```

```python
import functools

import jax
import jax.numpy as jnp
from jax import lax
from jax.experimental import pallas as pl
from jax.experimental.pallas import tpu as pltpu
from jax.sharding import Mesh
from jax.sharding import PartitionSpec as P

HD = 64
BLOCK = 64
EP = ("ep_0", "ep_1")
TP = ("tp_y", "tp_x")
EP_TP = ("ep_0", "ep_1", "tp_y", "tp_x")
EXPERTS = 32
CAP = 20
SLOT = 2 * CAP
GROUP = 8
LIMIT = 16 * 1024 * 1024


def iota(shape, dim):
    return lax.broadcasted_iota(jnp.int32, shape, dim)


def nt(a, b):
    return lax.dot_general(a, b, (((1,), (1,)), ((), ())), preferred_element_type=jnp.float32)


def mm(a, b):
    return jnp.dot(a, b, preferred_element_type=jnp.float32)


NN = (((1,), (0,)), ((), ()))
NT = (((1,), (1,)), ((), ()))
TN = (((0,), (0,)), ((), ()))


def halves(a):
    high = a.astype(jnp.bfloat16)
    return high, (a - high.astype(jnp.float32)).astype(jnp.bfloat16)


def dot(a, b, dims):
    return lax.dot_general(a, b, dims, preferred_element_type=jnp.float32)


def fine_dot(a, b, dims=NN):
    ah, al = halves(a)
    bh, bl = halves(b)
    return dot(ah, bh, dims) + dot(ah, bl, dims) + dot(al, bh, dims)


def call(kernel, outs, *args, scalars=0, scratch=(), limit=LIMIT):
    whole = [pl.BlockSpec(memory_space=pltpu.VMEM)] * (len(args) - scalars)
    return pl.pallas_call(
        kernel,
        out_shape=outs,
        in_specs=[pl.BlockSpec(memory_space=pltpu.SMEM)] * scalars + whole,
        scratch_shapes=list(scratch),
        compiler_params=pltpu.CompilerParams(vmem_limit_bytes=limit),
    )(*args)


def shape(dims, dtype=jnp.bfloat16):
    return jax.ShapeDtypeStruct(dims, dtype)


def prep_kernel(place, x, gain, routes, weights, out, rank_out, share_out):
    rows = x.shape[0]
    full = x[...].astype(jnp.float32)
    scale = lax.rsqrt(jnp.mean(full * full, axis=-1, keepdims=True) + 1.0)
    mine = pl.ds(pl.multiple_of(place[0] * 256, 256), 256)
    piece = (x[:, mine].astype(jnp.float32) * scale * gain[:, mine]).astype(jnp.bfloat16)
    w = weights[...]
    portion = w / jnp.sum(w, axis=0, keepdims=True)
    expert = iota((EXPERTS, rows), 0)
    chosen = jnp.zeros((EXPERTS, rows), jnp.float32)
    share = jnp.zeros((EXPERTS, rows), jnp.float32)
    for j in range(routes.shape[0]):
        hit = routes[j : j + 1, :] == expert
        chosen = jnp.where(hit, 1.0, chosen)
        share = jnp.where(hit, portion[j : j + 1, :], share)
    earlier = (iota((rows, rows), 0) <= iota((rows, rows), 1)).astype(jnp.bfloat16)
    rank = mm(chosen.astype(jnp.bfloat16), earlier) * chosen
    rank_out[...] = rank
    share_out[...] = share
    total = EXPERTS * SLOT
    q = iota((total, EXPERTS), 0)
    spread = (q // SLOT == iota((total, EXPERTS), 1)).astype(jnp.bfloat16)
    seat = (iota((total, rows), 0) % CAP + 1).astype(jnp.float32)
    pick = (mm(spread, rank.astype(jnp.bfloat16)) == seat).astype(jnp.bfloat16)
    both = mm(pick, piece)
    second = iota((total, 128), 0) % SLOT >= CAP
    out[...] = jnp.where(second, both[:, 128:], both[:, :128]).astype(jnp.bfloat16)


def combine_kernel(back, rank, share, out):
    rows = rank.shape[1]
    total = EXPERTS * SLOT
    rank = jnp.transpose(rank[...])
    share = jnp.transpose(share[...])
    spread = (iota((total, EXPERTS), 0) // SLOT == iota((total, EXPERTS), 1)).astype(jnp.bfloat16)
    q = iota((rows, total), 1)
    match = nt(rank.astype(jnp.bfloat16), spread) == (q % CAP + 1).astype(jnp.float32)
    second = q % SLOT >= CAP
    high, low = halves(share)
    values = back[...]
    first_half = jnp.zeros((rows, 128), jnp.float32)
    second_half = jnp.zeros((rows, 128), jnp.float32)
    for part in (high, low):
        wide = jnp.where(match, nt(part, spread), 0.0)
        first_half += mm(jnp.where(second, 0.0, wide).astype(jnp.bfloat16), values)
        second_half += mm(jnp.where(second, wide, 0.0).astype(jnp.bfloat16), values)
    out[:, :128] = first_half.astype(out.dtype)
    out[:, 128:] = second_half.astype(out.dtype)


def selector(half):
    r = iota((GROUP * CAP, GROUP * SLOT), 0)
    return (iota((GROUP * CAP, GROUP * SLOT), 1) == r // CAP * SLOT + r % CAP + half * CAP).astype(
        jnp.bfloat16
    )


def gate_up_kernel(place, gathered, w0, w1, w2, w3, out, weights, rows):
    pick = jnp.concatenate([selector(0), selector(1)], axis=0)
    side = weights.shape[0]
    for back, w in enumerate((w0, w1, w2, w3)):
        weights[(place[0] + side - back) % side] = w[: weights.shape[1], :]
    each = GROUP * CAP
    for g in range(EXPERTS // GROUP):
        for k in range(gathered.shape[0]):
            seen = gathered[k, g * GROUP * SLOT : (g + 1) * GROUP * SLOT, :]
            found = mm(pick, seen).astype(jnp.bfloat16)
            for half in range(2):
                at = (2 * k + half) * 128
                rows[g * each : (g + 1) * each, at : at + 128] = found[
                    half * each : (half + 1) * each
                ]
    whole = rows[...]
    for k in range(side // 2):
        pair = jnp.concatenate([weights[2 * k], weights[2 * k + 1]], axis=0)
        made = nt(whole, pair).astype(jnp.bfloat16)
        for g in range(EXPERTS // GROUP):
            out[g, :, k * 256 : (k + 1) * 256] = made[g * each : (g + 1) * each]


def hidden_kernel(parts, out):
    both = jnp.zeros(parts.shape[1:], jnp.float32)
    for k in range(parts.shape[0]):
        both += parts[k].astype(jnp.float32)
    made = []
    for k in range(both.shape[1] // 128):
        v = both[:, k * 128 : (k + 1) * 128]
        made.append(jax.nn.silu(v) * pltpu.roll(v, 64, 1))
    left = iota((both.shape[0], 128), 1) < 64
    for k in range(len(made) // 2):
        value = jnp.where(left, made[2 * k], pltpu.roll(made[2 * k + 1], 64, 1))
        for peer in range(out.shape[0]):
            out[peer, :, k * 128 : (k + 1) * 128] = value.astype(jnp.bfloat16)


def down_kernel(hidden, weights, out):
    picks = (selector(0), selector(1))
    side = 4
    tall = []
    for k in range(side):
        tall.append(
            jnp.concatenate(
                [weights[(side * m + k) * 64 : (side * m + k + 1) * 64, :] for m in range(side)], 0
            )
        )
    for g in range(side):
        total = mm(hidden[side * g], tall[0])
        for k in range(1, side):
            total += mm(hidden[side * g + k], tall[k])
        total = total.astype(jnp.bfloat16)
        placed = jnp.zeros((GROUP * SLOT, 128), jnp.float32)
        for half in range(2):
            placed += lax.dot_general(
                picks[half],
                total[:, half * 128 : (half + 1) * 128],
                (((0,), (0,)), ((), ())),
                preferred_element_type=jnp.float32,
            )
        out[g * GROUP * SLOT : (g + 1) * GROUP * SLOT, :] = placed.astype(jnp.bfloat16)


def exchanged(tiles, axis):
    return lax.all_to_all(tiles, axis, split_axis=0, concat_axis=0, tiled=True)


def head_sums(a):
    left = iota(a.shape, 1) < HD
    low = jnp.sum(jnp.where(left, a, 0.0), axis=-1, keepdims=True)
    high = jnp.sum(jnp.where(left, 0.0, a), axis=-1, keepdims=True)
    return jnp.where(left, low, high)


def tables_kernel(receptance, key_in, value_in, decay_in, rate_in, begun, send, table):
    f32 = jnp.float32
    size = (BLOCK, BLOCK)
    strict = (iota(size, 1) < iota(size, 0)).astype(f32)
    closed = (iota(size, 1) <= iota(size, 0)).astype(f32)
    eye = (iota(size, 1) == iota(size, 0)).astype(f32)
    summing = closed.astype(jnp.bfloat16)
    count = receptance.shape[0] // BLOCK
    heads = receptance.shape[1] // HD
    state = [jnp.concatenate([eye, jnp.zeros(size, f32)], axis=1) for _ in range(heads)]
    blocks = []
    for b in range(count):
        at = slice(b * BLOCK, (b + 1) * BLOCK)
        readout = receptance[at, :].astype(f32)
        key = key_in[at, :].astype(f32)
        value = value_in[at, :].astype(f32)
        log_decay = -jnp.exp(-jax.nn.softplus(-decay_in[at, :].astype(f32)) - 0.5)
        rate = jax.nn.sigmoid(rate_in[at, :].astype(f32))
        unit = key / jnp.sqrt(head_sums(key * key) + 1.0)
        first, _ = halves(log_decay)
        middle = (log_decay - first.astype(f32)).astype(jnp.bfloat16)
        last = (log_decay - first.astype(f32) - middle.astype(f32)).astype(jnp.bfloat16)
        inclusive = mm(summing, first) + mm(summing, middle) + mm(summing, last)
        total = inclusive[BLOCK - 1 :, :]
        probe = -unit * jnp.exp(inclusive - log_decay)
        removal = unit * rate
        written = key * rate
        grow = jnp.exp(-inclusive)
        tail = jnp.exp(total - inclusive)
        blocks.append(
            (
                probe,
                readout * jnp.exp(inclusive),
                removal * grow,
                written * grow,
                removal * tail,
                written * tail,
                value,
                jnp.exp(total),
            )
        )
    work = []
    for b in range(count):
        for h in range(heads):
            side = slice(h * HD, (h + 1) * HD)
            cut = [a[:, side] for a in blocks[b]]
            probe, readout, removal, written, removal_tail, written_tail, value, total = cut
            meet = fine_dot(
                jnp.concatenate([probe, readout], 0), jnp.concatenate([removal, written], 0), NT
            )
            work.append(
                dict(
                    lower=meet[:BLOCK, :BLOCK] * strict,
                    write=meet[:BLOCK, BLOCK:] * strict,
                    reach=meet[BLOCK:, :BLOCK] * closed,
                    reach_write=meet[BLOCK:, BLOCK:] * closed,
                    probe=probe,
                    readout=readout,
                    removal_tail=removal_tail,
                    written_tail=written_tail,
                    value=value,
                    total=total,
                )
            )
    inverses = [eye + w["lower"] for w in work]
    powers = [fine_dot(w["lower"], w["lower"]) for w in work]
    for step in range(BLOCK.bit_length() - 2):
        for k in range(len(work)):
            if step + 3 < BLOCK.bit_length():
                both = fine_dot(jnp.concatenate([inverses[k], powers[k]], 0), powers[k])
                inverses[k] = inverses[k] + both[:BLOCK]
                powers[k] = both[BLOCK:]
            else:
                inverses[k] = inverses[k] + fine_dot(inverses[k], powers[k])
    zero = jnp.zeros(size, f32)
    steps = []
    for k, w in enumerate(work):
        seen = fine_dot(w["write"], w["value"])
        solved = fine_dot(inverses[k], jnp.concatenate([w["probe"], seen], 1))
        right = jnp.concatenate([solved, jnp.concatenate([zero, w["value"]], 1)], 0)
        moved = fine_dot(jnp.concatenate([w["removal_tail"], w["written_tail"]], 0), right, TN)
        heard = fine_dot(jnp.concatenate([w["reach"], w["reach_write"]], 1), right)
        steps.append(
            (
                jnp.concatenate([w["readout"] + heard[:, :HD], eye * w["total"] + moved[:, :HD]], 0),
                jnp.concatenate([heard[:, HD:], moved[:, HD:]], 0),
            )
        )
    for b in range(count):
        at = slice(b * BLOCK, (b + 1) * BLOCK)
        reads = []
        locals_ = []
        for h in range(heads):
            maps, adds = steps[b * heads + h]
            new = fine_dot(maps, state[h])
            added = new[:, HD:] + adds
            reads.append(new[:BLOCK, :HD])
            locals_.append(added[:BLOCK])
            state[h] = jnp.concatenate([new[BLOCK:, :HD], added[BLOCK:]], 1)
        table[0, at, :] = jnp.concatenate(reads, 1)
        table[1, at, :] = jnp.concatenate(locals_, 1)
    for h in range(heads):
        begun[h, :HD] = state[h]
        begun[h, HD:] = jnp.concatenate([eye, zero], 1)
        send[h] = state[h].astype(jnp.bfloat16)


def advanced(later, came, old):
    right = iota(old.shape, 1) >= HD
    high, low = halves(old[:, :HD])
    new = mm(high, came) + mm(low, came) + jnp.where(right, old, 0.0)
    return jnp.where(later, new, old)


def round_kernel(position, came, state, state_out, send_out, *, shift):
    for h in range(state.shape[0]):
        new = advanced(position[0] >= shift, came[h], state[h])
        state_out[h] = new
        if len(send_out.shape) == 3:
            send_out[h] = new[:HD].astype(jnp.bfloat16)
        else:
            send_out[:, h * HD : (h + 1) * HD] = new[:HD, HD:].astype(jnp.bfloat16)


def readout_kernel(position, came, last, table, gain, out, *, shift):
    later = position[0] >= shift
    states = []
    for h in range(last.shape[0]):
        side = slice(h * HD, (h + 1) * HD)
        old = last[h, HD:, :]
        high, low = halves(old[:, :HD])
        new = mm(high, came[:, side]) + mm(low, came[:, side]) + old[:, HD:]
        states.append(jnp.where(later, new, old[:, HD:]))
    first, second = states
    zero = jnp.zeros_like(first)
    state = jnp.concatenate(
        [jnp.concatenate([first, zero], 1), jnp.concatenate([zero, second], 1)], 0
    )
    seen = fine_dot(table[0], state) + table[1]
    center = seen - head_sums(seen) / HD
    spread = head_sums(center * center) / HD
    out[...] = (center * lax.rsqrt(spread + 1.0) * gain[...]).astype(jnp.bfloat16)


def copies_kernel(one, out):
    for k in range(out.shape[0]):
        out[k] = one[...]


def pack_kernel(place, gate, up, out_weight, p0, p1, p2, p3):
    side = 4
    hidden, features = gate.shape
    length = features // side
    for ahead, p in enumerate((p0, p1, p2, p3)):
        target = (place[0] + ahead) % side
        at = pl.ds(pl.multiple_of(target * length, length), length)
        p[:hidden, :] = gate[:, at]
        p[hidden : 2 * hidden, :] = up[:, at]
        p[2 * hidden :, :] = out_weight[:, at]


def product_kernel(place, m0, m1, m2, m3, w0, w1, w2, w3, p0, p1, p2, p3, made):
    rows = jnp.concatenate([m[...] for m in (m0, m1, m2, m3)], 1)
    count = rows.shape[1] // 4
    weights = jnp.concatenate([w[w.shape[0] - count :, :] for w in (w0, w1, w2, w3)], 0)
    whole = mm(rows, weights).astype(jnp.bfloat16)
    peers, each, _ = made.shape
    for p in range(peers):
        made[p] = whole[p * each : (p + 1) * each]
    side = p0.shape[0]
    for ahead, part in enumerate((p0, p1, p2, p3)):
        for y in range(side):
            part[y] = made[side * y + (place[0] + ahead) % side]


def adding_kernel(p0, p1, p2, p3, out):
    for y in range(out.shape[0]):
        total = p0[y].astype(jnp.float32) + p1[y].astype(jnp.float32)
        total += p2[y].astype(jnp.float32) + p3[y].astype(jnp.float32)
        out[y] = total.astype(jnp.bfloat16)


def finish_kernel(tiles, out):
    side, _, width = tiles.shape
    for y in range(side):
        out[:, y * width : (y + 1) * width] = tiles[y]


def turned(shard, axis, back):
    n = lax.axis_size(axis)
    return lax.ppermute(shard, axis, [(i, (i + back) % n) for i in range(n)])


def local(
    receptance,
    key_in,
    value_in,
    decay_in,
    rate_in,
    norm_gain,
    out_weight,
    moe_in,
    ffn_gain,
    routes,
    route_weights,
    gate_weight,
    up_weight,
    down_weight,
):
    f32 = jnp.float32
    rows, features = moe_in.shape
    tp = lax.axis_size(TP)
    side = lax.axis_size("tp_y")
    width = features // tp
    column_place = lax.axis_index("tp_x").astype(jnp.int32).reshape(1)
    row_place = lax.axis_index("tp_y").astype(jnp.int32).reshape(1)
    total = EXPERTS * SLOT
    share_rows = EXPERTS * CAP // side
    outgoing, rank, share = call(
        prep_kernel,
        (shape((total, 128)), shape((EXPERTS, rows), f32), shape((EXPERTS, rows), f32)),
        lax.axis_index(TP).astype(jnp.int32).reshape(1),
        moe_in,
        ffn_gain.reshape(1, features),
        routes.T,
        route_weights.T,
        scalars=1,
        limit=None,
    )
    arrived = exchanged(outgoing.reshape(EXPERTS, SLOT, 128), EP)
    packs = call(
        pack_kernel,
        [shape((256, features // side))] * side,
        row_place,
        gate_weight[0].T,
        up_weight[0].T,
        out_weight,
        scalars=1,
    )
    moved = [packs[0]] + [turned(packs[k], "tp_y", k) for k in range(1, side)]

    tokens, columns = receptance.shape
    heads = columns // HD
    pack = (heads, HD, 2 * HD)
    stack = (heads, 2 * HD, 2 * HD)
    flat = (tokens, columns)
    state, send, table = call(
        tables_kernel,
        (shape(stack, f32), shape(pack), shape((2, *flat), f32)),
        receptance,
        key_in,
        value_in,
        decay_in,
        rate_in,
    )
    peers = lax.axis_size(EP)
    position = lax.axis_index(EP).astype(jnp.int32).reshape(1)
    shift = 1
    while shift < peers:
        came = lax.ppermute(send, EP, [(i, i + shift) for i in range(peers - shift)])
        if 2 * shift < peers:
            state, send = call(
                functools.partial(round_kernel, shift=shift),
                (shape(stack, f32), shape(pack if 4 * shift < peers else (HD, 2 * HD))),
                position,
                came,
                state,
                scalars=1,
            )
        shift = 2 * shift
    mixed = call(
        functools.partial(readout_kernel, shift=shift // 2),
        shape(flat),
        position,
        came,
        state,
        table,
        norm_gain.reshape(1, columns),
        scalars=1,
    )
    mixes = [mixed] + [turned(mixed, "tp_y", k) for k in range(1, side)]
    quarter = (side, tokens // tp, features // side)
    products = call(
        product_kernel,
        [shape(quarter)] * side,
        column_place,
        *mixes,
        *moved,
        scalars=1,
        scratch=[pltpu.VMEM((tp, *quarter[1:]), jnp.bfloat16)],
    )
    shares = [products[0]] + [turned(products[k], "tp_x", k) for k in range(1, side)]
    added = call(adding_kernel, shape(quarter), *shares)

    copies = call(
        copies_kernel, shape((side, total, 128)), arrived.reshape(total, 128)
    )
    gathered = exchanged(copies, "tp_x")
    wide = side * 128
    partial = call(
        gate_up_kernel,
        shape((side, share_rows, wide)),
        row_place,
        gathered,
        *moved,
        scalars=1,
        scratch=[
            pltpu.VMEM((side, 128, features // side), jnp.bfloat16),
            pltpu.VMEM((EXPERTS * CAP, features // side), jnp.bfloat16),
        ],
    )
    parts = exchanged(partial, "tp_y")
    hidden = call(hidden_kernel, shape((tp, share_rows, wide // 2)), parts)
    everyone = exchanged(hidden, TP)
    result = call(down_kernel, shape((total, 128)), everyone, down_weight[0])
    returned = exchanged(result.reshape(EXPERTS, SLOT, 128), EP)
    tiles = exchanged(added, "tp_y")
    moe_out = call(combine_kernel, shape((rows, width)), returned.reshape(total, 128), rank, share)
    mixer_out = call(finish_kernel, shape((tokens // tp, features)), tiles)
    return (mixer_out, moe_out)


def solution(mesh):
    finer = Mesh(mesh.devices.reshape(16, 2, 4, 4), EP_TP)
    placed = (
        P(EP, TP),
        P(EP, TP),
        P(EP, TP),
        P(EP, TP),
        P(EP, TP),
        P(TP),
        P(TP, None),
        P(EP, None),
        P(),
        P(EP, None),
        P(EP, None),
        P(EP, None, TP),
        P(EP, None, TP),
        P(EP, None, TP),
    )
    return jax.shard_map(
        local, mesh=finer, in_specs=placed, out_specs=(P(EP_TP, None), P(EP, TP)), check_vma=False
    )
```

```python
import functools

import jax
import jax.numpy as jnp
from jax import lax
from jax.experimental import pallas as pl
from jax.experimental.pallas import tpu as pltpu
from jax.sharding import Mesh
from jax.sharding import PartitionSpec as P

HD = 64
BLOCK = 64
EP = ("ep_0", "ep_1")
TP = ("tp_y", "tp_x")
EP_TP = ("ep_0", "ep_1", "tp_y", "tp_x")
EXPERTS = 32
CAP = 20
SLOT = 2 * CAP
GROUP = 8
LIMIT = 16 * 1024 * 1024


def iota(shape, dim):
    return lax.broadcasted_iota(jnp.int32, shape, dim)


def nt(a, b):
    return lax.dot_general(a, b, (((1,), (1,)), ((), ())), preferred_element_type=jnp.float32)


def mm(a, b):
    return jnp.dot(a, b, preferred_element_type=jnp.float32)


NN = (((1,), (0,)), ((), ()))
NT = (((1,), (1,)), ((), ()))
TN = (((0,), (0,)), ((), ()))


def halves(a):
    high = a.astype(jnp.bfloat16)
    return high, (a - high.astype(jnp.float32)).astype(jnp.bfloat16)


def dot(a, b, dims):
    return lax.dot_general(a, b, dims, preferred_element_type=jnp.float32)


def fine_dot(a, b, dims=NN):
    ah, al = halves(a)
    bh, bl = halves(b)
    return dot(ah, bh, dims) + dot(ah, bl, dims) + dot(al, bh, dims)


def call(kernel, outs, *args, scalars=0, scratch=(), limit=LIMIT, space=pltpu.SMEM):
    whole = [pl.BlockSpec(memory_space=pltpu.VMEM)] * (len(args) - scalars)
    return pl.pallas_call(
        kernel,
        out_shape=outs,
        in_specs=[pl.BlockSpec(memory_space=space)] * scalars + whole,
        scratch_shapes=list(scratch),
        compiler_params=pltpu.CompilerParams(vmem_limit_bytes=limit),
    )(*args)


def shape(dims, dtype=jnp.bfloat16):
    return jax.ShapeDtypeStruct(dims, dtype)


def prep_kernel(place, x, gain, routes, weights, out, rank_out, share_out):
    rows = x.shape[0]
    full = x[...].astype(jnp.float32)
    scale = lax.rsqrt(jnp.mean(full * full, axis=-1, keepdims=True) + 1.0)
    mine = pl.ds(pl.multiple_of(place[0] * 256, 256), 256)
    piece = (x[:, mine].astype(jnp.float32) * scale * gain[:, mine]).astype(jnp.bfloat16)
    w = weights[...]
    portion = w / jnp.sum(w, axis=0, keepdims=True)
    expert = iota((EXPERTS, rows), 0)
    chosen = jnp.zeros((EXPERTS, rows), jnp.float32)
    share = jnp.zeros((EXPERTS, rows), jnp.float32)
    for j in range(routes.shape[0]):
        hit = routes[j : j + 1, :] == expert
        chosen = jnp.where(hit, 1.0, chosen)
        share = jnp.where(hit, portion[j : j + 1, :], share)
    earlier = (iota((rows, rows), 0) <= iota((rows, rows), 1)).astype(jnp.bfloat16)
    rank = mm(chosen.astype(jnp.bfloat16), earlier) * chosen
    rank_out[...] = rank
    share_out[...] = share
    total = EXPERTS * SLOT
    q = iota((total, EXPERTS), 0)
    spread = (q // SLOT == iota((total, EXPERTS), 1)).astype(jnp.bfloat16)
    seat = (iota((total, rows), 0) % CAP + 1).astype(jnp.float32)
    pick = (mm(spread, rank.astype(jnp.bfloat16)) == seat).astype(jnp.bfloat16)
    both = mm(pick, piece)
    second = iota((total, 128), 0) % SLOT >= CAP
    out[...] = jnp.where(second, both[:, 128:], both[:, :128]).astype(jnp.bfloat16)


def combine_kernel(back, rank, share, out):
    rows = rank.shape[1]
    total = EXPERTS * SLOT
    rank = jnp.transpose(rank[...])
    share = jnp.transpose(share[...])
    spread = (iota((total, EXPERTS), 0) // SLOT == iota((total, EXPERTS), 1)).astype(jnp.bfloat16)
    q = iota((rows, total), 1)
    match = nt(rank.astype(jnp.bfloat16), spread) == (q % CAP + 1).astype(jnp.float32)
    second = q % SLOT >= CAP
    high, low = halves(share)
    values = back[...]
    first_half = jnp.zeros((rows, 128), jnp.float32)
    second_half = jnp.zeros((rows, 128), jnp.float32)
    for part in (high, low):
        wide = jnp.where(match, nt(part, spread), 0.0)
        first_half += mm(jnp.where(second, 0.0, wide).astype(jnp.bfloat16), values)
        second_half += mm(jnp.where(second, wide, 0.0).astype(jnp.bfloat16), values)
    out[:, :128] = first_half.astype(out.dtype)
    out[:, 128:] = second_half.astype(out.dtype)


def selector(half):
    r = iota((GROUP * CAP, GROUP * SLOT), 0)
    return (iota((GROUP * CAP, GROUP * SLOT), 1) == r // CAP * SLOT + r % CAP + half * CAP).astype(
        jnp.bfloat16
    )


def gate_up_kernel(place, gathered, w0, w1, w2, w3, out, weights, rows):
    pick = jnp.concatenate([selector(0), selector(1)], axis=0)
    side = weights.shape[0]
    for back, w in enumerate((w0, w1, w2, w3)):
        weights[(place[0] + side - back) % side] = w[: weights.shape[1], :]
    each = GROUP * CAP
    for g in range(EXPERTS // GROUP):
        for k in range(gathered.shape[0]):
            seen = gathered[k, g * GROUP * SLOT : (g + 1) * GROUP * SLOT, :]
            found = mm(pick, seen).astype(jnp.bfloat16)
            for half in range(2):
                at = (2 * k + half) * 128
                rows[g * each : (g + 1) * each, at : at + 128] = found[
                    half * each : (half + 1) * each
                ]
    whole = rows[...]
    for k in range(side // 2):
        pair = jnp.concatenate([weights[2 * k], weights[2 * k + 1]], axis=0)
        made = nt(whole, pair).astype(jnp.bfloat16)
        for g in range(EXPERTS // GROUP):
            out[g, :, k * 256 : (k + 1) * 256] = made[g * each : (g + 1) * each]


def hidden_kernel(parts, out):
    both = jnp.zeros(parts.shape[1:], jnp.float32)
    for k in range(parts.shape[0]):
        both += parts[k].astype(jnp.float32)
    made = []
    for k in range(both.shape[1] // 128):
        v = both[:, k * 128 : (k + 1) * 128]
        made.append(jax.nn.silu(v) * pltpu.roll(v, 64, 1))
    left = iota((both.shape[0], 128), 1) < 64
    for k in range(len(made) // 2):
        value = jnp.where(left, made[2 * k], pltpu.roll(made[2 * k + 1], 64, 1))
        for peer in range(out.shape[0]):
            out[peer, :, k * 128 : (k + 1) * 128] = value.astype(jnp.bfloat16)


def down_kernel(stored, hidden, out, weights, done):
    fetch = pltpu.make_async_copy(stored, weights, done)
    fetch.start()
    picks = (selector(0), selector(1))
    fetch.wait()
    side = 4
    tall = []
    for k in range(side):
        tall.append(
            jnp.concatenate(
                [weights[(side * m + k) * 64 : (side * m + k + 1) * 64, :] for m in range(side)], 0
            )
        )
    for g in range(side):
        total = mm(hidden[side * g], tall[0])
        for k in range(1, side):
            total += mm(hidden[side * g + k], tall[k])
        total = total.astype(jnp.bfloat16)
        placed = jnp.zeros((GROUP * SLOT, 128), jnp.float32)
        for half in range(2):
            placed += lax.dot_general(
                picks[half],
                total[:, half * 128 : (half + 1) * 128],
                (((0,), (0,)), ((), ())),
                preferred_element_type=jnp.float32,
            )
        out[g * GROUP * SLOT : (g + 1) * GROUP * SLOT, :] = placed.astype(jnp.bfloat16)


def exchanged(tiles, axis):
    return lax.all_to_all(tiles, axis, split_axis=0, concat_axis=0, tiled=True)


def head_sums(a):
    left = iota(a.shape, 1) < HD
    low = jnp.sum(jnp.where(left, a, 0.0), axis=-1, keepdims=True)
    high = jnp.sum(jnp.where(left, 0.0, a), axis=-1, keepdims=True)
    return jnp.where(left, low, high)


def tables_kernel(receptance, key_in, value_in, decay_in, rate_in, begun, send, table):
    f32 = jnp.float32
    size = (BLOCK, BLOCK)
    strict = (iota(size, 1) < iota(size, 0)).astype(f32)
    closed = (iota(size, 1) <= iota(size, 0)).astype(f32)
    eye = (iota(size, 1) == iota(size, 0)).astype(f32)
    summing = closed.astype(jnp.bfloat16)
    count = receptance.shape[0] // BLOCK
    heads = receptance.shape[1] // HD
    state = [jnp.concatenate([eye, jnp.zeros(size, f32)], axis=1) for _ in range(heads)]
    blocks = []
    for b in range(count):
        at = slice(b * BLOCK, (b + 1) * BLOCK)
        readout = receptance[at, :].astype(f32)
        key = key_in[at, :].astype(f32)
        value = value_in[at, :].astype(f32)
        log_decay = -jnp.exp(-jax.nn.softplus(-decay_in[at, :].astype(f32)) - 0.5)
        rate = jax.nn.sigmoid(rate_in[at, :].astype(f32))
        unit = key / jnp.sqrt(head_sums(key * key) + 1.0)
        first, _ = halves(log_decay)
        middle = (log_decay - first.astype(f32)).astype(jnp.bfloat16)
        last = (log_decay - first.astype(f32) - middle.astype(f32)).astype(jnp.bfloat16)
        inclusive = mm(summing, first) + mm(summing, middle) + mm(summing, last)
        total = inclusive[BLOCK - 1 :, :]
        probe = -unit * jnp.exp(inclusive - log_decay)
        removal = unit * rate
        written = key * rate
        grow = jnp.exp(-inclusive)
        tail = jnp.exp(total - inclusive)
        blocks.append(
            (
                probe,
                readout * jnp.exp(inclusive),
                removal * grow,
                written * grow,
                removal * tail,
                written * tail,
                value,
                jnp.exp(total),
            )
        )
    work = []
    for b in range(count):
        for h in range(heads):
            side = slice(h * HD, (h + 1) * HD)
            cut = [a[:, side] for a in blocks[b]]
            probe, readout, removal, written, removal_tail, written_tail, value, total = cut
            meet = fine_dot(
                jnp.concatenate([probe, readout], 0), jnp.concatenate([removal, written], 0), NT
            )
            work.append(
                dict(
                    lower=meet[:BLOCK, :BLOCK] * strict,
                    write=meet[:BLOCK, BLOCK:] * strict,
                    reach=meet[BLOCK:, :BLOCK] * closed,
                    reach_write=meet[BLOCK:, BLOCK:] * closed,
                    probe=probe,
                    readout=readout,
                    removal_tail=removal_tail,
                    written_tail=written_tail,
                    value=value,
                    total=total,
                )
            )
    inverses = [eye + w["lower"] for w in work]
    powers = [fine_dot(w["lower"], w["lower"]) for w in work]
    for step in range(BLOCK.bit_length() - 2):
        for k in range(len(work)):
            if step + 3 < BLOCK.bit_length():
                both = fine_dot(jnp.concatenate([inverses[k], powers[k]], 0), powers[k])
                inverses[k] = inverses[k] + both[:BLOCK]
                powers[k] = both[BLOCK:]
            else:
                inverses[k] = inverses[k] + fine_dot(inverses[k], powers[k])
    zero = jnp.zeros(size, f32)
    steps = []
    for k, w in enumerate(work):
        seen = fine_dot(w["write"], w["value"])
        solved = fine_dot(inverses[k], jnp.concatenate([w["probe"], seen], 1))
        right = jnp.concatenate([solved, jnp.concatenate([zero, w["value"]], 1)], 0)
        moved = fine_dot(jnp.concatenate([w["removal_tail"], w["written_tail"]], 0), right, TN)
        heard = fine_dot(jnp.concatenate([w["reach"], w["reach_write"]], 1), right)
        steps.append(
            (
                jnp.concatenate([w["readout"] + heard[:, :HD], eye * w["total"] + moved[:, :HD]], 0),
                jnp.concatenate([heard[:, HD:], moved[:, HD:]], 0),
            )
        )
    for b in range(count):
        at = slice(b * BLOCK, (b + 1) * BLOCK)
        reads = []
        locals_ = []
        for h in range(heads):
            maps, adds = steps[b * heads + h]
            new = fine_dot(maps, state[h])
            added = new[:, HD:] + adds
            reads.append(new[:BLOCK, :HD])
            locals_.append(added[:BLOCK])
            state[h] = jnp.concatenate([new[BLOCK:, :HD], added[BLOCK:]], 1)
        table[0, at, :] = jnp.concatenate(reads, 1)
        table[1, at, :] = jnp.concatenate(locals_, 1)
    for h in range(heads):
        begun[h, :HD] = state[h]
        begun[h, HD:] = jnp.concatenate([eye, zero], 1)
        send[h] = state[h].astype(jnp.bfloat16)


def advanced(later, came, old):
    right = iota(old.shape, 1) >= HD
    high, low = halves(old[:, :HD])
    new = mm(high, came) + mm(low, came) + jnp.where(right, old, 0.0)
    return jnp.where(later, new, old)


def round_kernel(position, came, state, state_out, send_out, *, shift):
    for h in range(state.shape[0]):
        new = advanced(position[0] >= shift, came[h], state[h])
        state_out[h] = new
        if len(send_out.shape) == 3:
            send_out[h] = new[:HD].astype(jnp.bfloat16)
        else:
            send_out[:, h * HD : (h + 1) * HD] = new[:HD, HD:].astype(jnp.bfloat16)


def readout_kernel(position, came, last, table, gain, out, *, shift):
    later = position[0] >= shift
    states = []
    for h in range(last.shape[0]):
        side = slice(h * HD, (h + 1) * HD)
        old = last[h, HD:, :]
        high, low = halves(old[:, :HD])
        new = mm(high, came[:, side]) + mm(low, came[:, side]) + old[:, HD:]
        states.append(jnp.where(later, new, old[:, HD:]))
    first, second = states
    zero = jnp.zeros_like(first)
    state = jnp.concatenate(
        [jnp.concatenate([first, zero], 1), jnp.concatenate([zero, second], 1)], 0
    )
    seen = fine_dot(table[0], state) + table[1]
    center = seen - head_sums(seen) / HD
    spread = head_sums(center * center) / HD
    out[...] = (center * lax.rsqrt(spread + 1.0) * gain[...]).astype(jnp.bfloat16)


def copies_kernel(one, out):
    for k in range(out.shape[0]):
        out[k] = one[...]


def pack_kernel(place, gate, up, out_weight, p0, p1, p2, p3):
    side = 4
    hidden, features = gate.shape
    length = features // side
    for ahead, p in enumerate((p0, p1, p2, p3)):
        target = (place[0] + ahead) % side
        at = pl.ds(pl.multiple_of(target * length, length), length)
        p[:hidden, :] = gate[:, at]
        p[hidden : 2 * hidden, :] = up[:, at]
        p[2 * hidden :, :] = out_weight[:, at]


def product_kernel(place, m0, m1, m2, m3, w0, w1, w2, w3, p0, p1, p2, p3, made):
    rows = jnp.concatenate([m[...] for m in (m0, m1, m2, m3)], 1)
    count = rows.shape[1] // 4
    weights = jnp.concatenate([w[w.shape[0] - count :, :] for w in (w0, w1, w2, w3)], 0)
    whole = mm(rows, weights).astype(jnp.bfloat16)
    peers, each, _ = made.shape
    for p in range(peers):
        made[p] = whole[p * each : (p + 1) * each]
    side = p0.shape[0]
    for ahead, part in enumerate((p0, p1, p2, p3)):
        for y in range(side):
            part[y] = made[side * y + (place[0] + ahead) % side]


def adding_kernel(p0, p1, p2, p3, out):
    for y in range(out.shape[0]):
        total = p0[y].astype(jnp.float32) + p1[y].astype(jnp.float32)
        total += p2[y].astype(jnp.float32) + p3[y].astype(jnp.float32)
        out[y] = total.astype(jnp.bfloat16)


def finish_kernel(tiles, out):
    side, _, width = tiles.shape
    for y in range(side):
        out[:, y * width : (y + 1) * width] = tiles[y]


def turned(shard, axis, back):
    n = lax.axis_size(axis)
    return lax.ppermute(shard, axis, [(i, (i + back) % n) for i in range(n)])


def local(
    receptance,
    key_in,
    value_in,
    decay_in,
    rate_in,
    norm_gain,
    out_weight,
    moe_in,
    ffn_gain,
    routes,
    route_weights,
    gate_weight,
    up_weight,
    down_weight,
):
    f32 = jnp.float32
    rows, features = moe_in.shape
    tp = lax.axis_size(TP)
    side = lax.axis_size("tp_y")
    width = features // tp
    column_place = lax.axis_index("tp_x").astype(jnp.int32).reshape(1)
    row_place = lax.axis_index("tp_y").astype(jnp.int32).reshape(1)
    total = EXPERTS * SLOT
    share_rows = EXPERTS * CAP // side
    outgoing, rank, share = call(
        prep_kernel,
        (shape((total, 128)), shape((EXPERTS, rows), f32), shape((EXPERTS, rows), f32)),
        lax.axis_index(TP).astype(jnp.int32).reshape(1),
        moe_in,
        ffn_gain.reshape(1, features),
        routes.T,
        route_weights.T,
        scalars=1,
        limit=None,
    )
    arrived = exchanged(outgoing.reshape(EXPERTS, SLOT, 128), EP)
    packs = call(
        pack_kernel,
        [shape((256, features // side))] * side,
        row_place,
        gate_weight[0].T,
        up_weight[0].T,
        out_weight,
        scalars=1,
    )
    moved = [packs[0]] + [turned(packs[k], "tp_y", k) for k in range(1, side)]

    tokens, columns = receptance.shape
    heads = columns // HD
    pack = (heads, HD, 2 * HD)
    stack = (heads, 2 * HD, 2 * HD)
    flat = (tokens, columns)
    state, send, table = call(
        tables_kernel,
        (shape(stack, f32), shape(pack), shape((2, *flat), f32)),
        receptance,
        key_in,
        value_in,
        decay_in,
        rate_in,
    )
    peers = lax.axis_size(EP)
    position = lax.axis_index(EP).astype(jnp.int32).reshape(1)
    shift = 1
    while shift < peers:
        came = lax.ppermute(send, EP, [(i, i + shift) for i in range(peers - shift)])
        if 2 * shift < peers:
            state, send = call(
                functools.partial(round_kernel, shift=shift),
                (shape(stack, f32), shape(pack if 4 * shift < peers else (HD, 2 * HD))),
                position,
                came,
                state,
                scalars=1,
            )
        shift = 2 * shift
    mixed = call(
        functools.partial(readout_kernel, shift=shift // 2),
        shape(flat),
        position,
        came,
        state,
        table,
        norm_gain.reshape(1, columns),
        scalars=1,
    )
    mixes = [mixed] + [turned(mixed, "tp_y", k) for k in range(1, side)]
    quarter = (side, tokens // tp, features // side)
    products = call(
        product_kernel,
        [shape(quarter)] * side,
        column_place,
        *mixes,
        *moved,
        scalars=1,
        scratch=[pltpu.VMEM((tp, *quarter[1:]), jnp.bfloat16)],
    )
    shares = [products[0]] + [turned(products[k], "tp_x", k) for k in range(1, side)]
    added = call(adding_kernel, shape(quarter), *shares)

    copies = call(
        copies_kernel, shape((side, total, 128)), arrived.reshape(total, 128)
    )
    gathered = exchanged(copies, "tp_x")
    wide = side * 128
    partial = call(
        gate_up_kernel,
        shape((side, share_rows, wide)),
        row_place,
        gathered,
        *moved,
        scalars=1,
        scratch=[
            pltpu.VMEM((side, 128, features // side), jnp.bfloat16),
            pltpu.VMEM((EXPERTS * CAP, features // side), jnp.bfloat16),
        ],
    )
    parts = exchanged(partial, "tp_y")
    hidden = call(hidden_kernel, shape((tp, share_rows, wide // 2)), parts)
    everyone = exchanged(hidden, TP)
    result = call(
        down_kernel,
        shape((total, 128)),
        down_weight[0],
        everyone,
        scalars=1,
        space=pl.ANY,
        scratch=[
            pltpu.VMEM(down_weight.shape[1:], jnp.bfloat16),
            pltpu.SemaphoreType.DMA(()),
        ],
    )
    returned = exchanged(result.reshape(EXPERTS, SLOT, 128), EP)
    tiles = exchanged(added, "tp_y")
    moe_out = call(combine_kernel, shape((rows, width)), returned.reshape(total, 128), rank, share)
    mixer_out = call(finish_kernel, shape((tokens // tp, features)), tiles)
    return (mixer_out, moe_out)


def solution(mesh):
    finer = Mesh(mesh.devices.reshape(16, 2, 4, 4), EP_TP)
    placed = (
        P(EP, TP),
        P(EP, TP),
        P(EP, TP),
        P(EP, TP),
        P(EP, TP),
        P(TP),
        P(TP, None),
        P(EP, None),
        P(),
        P(EP, None),
        P(EP, None),
        P(EP, None, TP),
        P(EP, None, TP),
        P(EP, None, TP),
    )
    return jax.shard_map(
        local, mesh=finer, in_specs=placed, out_specs=(P(EP_TP, None), P(EP, TP)), check_vma=False
    )
```
